32 devices in a mesh: grp: 2 (over y), fs: 4 (over z), tp: 4 (over x, core).
Axes of the slice: x: 2, y: 2, z: 4, core: 2. Of those that a mesh axis runs over, the one named last changes fastest.
Arguments:
- tokens: bfloat16 [2560, 2048], P(('grp', 'fs', 'tp')), parts along dimension 0, may hold values from -6 to 6
- mix_gain: bfloat16 [2048], replicated, may hold values from 0.099609375 to 1.8984375
- val_weight: bfloat16 [2048, 1024], P('fs', 'tp'), may hold values from -4 to 4
- gate_weight: bfloat16 [2048, 1024], P('fs', 'tp'), may hold values from -0.125 to 0.125
- conv_taps: bfloat16 [31, 1024], replicated, may hold values from -1 to 1
- chan_gain: bfloat16 [1024], replicated, may hold values from 0.099609375 to 1.8984375
- out_weight: bfloat16 [1024, 2048], P('tp', 'fs'), may hold values from -0.1875 to 0.1875
- mix_post_gain: bfloat16 [2048], replicated, may hold values from 0.099609375 to 1.8984375
- ffn_gain: bfloat16 [2048], replicated, may hold values from 0.099609375 to 1.8984375
- up_gate_weight: bfloat16 [2048, 5120], P('fs', 'tp'), may hold values from -0.125 to 0.125
- up_val_weight: bfloat16 [2048, 5120], P('fs', 'tp'), may hold values from -0.125 to 0.125
- ffn_taps: bfloat16 [2, 3, 5120], replicated, may hold values from -3.5 to 3.5
- down_weight: bfloat16 [5120, 2048], P('tp', 'fs'), may hold values from -0.078125 to 0.078125
- ffn_post_gain: bfloat16 [2048], replicated, may hold values from 0.099609375 to 1.8984375
Outputs:
- layer_out: bfloat16 [2560, 2048], P(('grp', 'fs', 'tp')), parts along dimension 0
The draws below stay inside these ranges and needn't reach their ends.
There are 2 independent parts, one for each index of `grp`. The reference program is written for one: setup_inputs(seed, part) draws one part's arguments, and reference() takes and returns one part's arrays. A program takes and returns all parts, laid end to end along the dimension named above; an argument that names none is the same for every part. Nothing has to cross between parts.
All inputs are finite; a program needn't handle non-finite values.
Results may differ from the reference program's by a relative error of at most 0.019.
Values may be sent and summed in bfloat16 or wider, within the bound.
A program may use at most 64 MiB of HBM per device.

```python
import jax
import jax.numpy as jnp
from jax import lax

D = 2048
CH = 1024
FF = 5120
CONV_TAPS = 31
FFN_TAPS = 3
LEN = 64
TOKENS = 1280
N_TP = 4


def draw_val_weight(key, part):
    base_key, rough_key = jax.random.split(key, 2)
    base_draw = jax.random.normal(base_key, (D, CH), jnp.float32) * D ** (-0.5)
    roughness = jnp.exp(jax.random.uniform(rough_key, (CH,), jnp.float32, -0.7, 0.7))
    position = jnp.arange(CH, dtype=jnp.float32) / CH
    drawn_values = base_draw * 4.0 ** position * roughness
    return jnp.clip(drawn_values, -4.0, 4.0).astype(jnp.bfloat16)


def shard_levels(rng, dims, pieces, smallest, top_value):
    level = 1.0
    for dim, shards_of in pieces:
        steps = jax.random.uniform(jax.random.fold_in(jax.random.fold_in(rng, 6), dim), (shards_of,), jnp.float32, smallest / len(pieces), top_value / len(pieces))
        level = level * jnp.repeat(jnp.exp(steps), dims[dim] // shards_of).reshape((-1,) + (1,) * (len(dims) - 1 - dim))
    return level


def gaussian(rng, shape, scale, most, cuts=(), held_as=jnp.bfloat16):
    values = jax.random.normal(rng, shape, jnp.float32) * scale
    if len(cuts) > 0:
        values = shard_levels(rng, shape, cuts, -0.22, 0.18) * values
    return jnp.clip(values, min=-most, max=most).astype(held_as)


def setup_inputs(seed: int = 0, part: int = 0) -> dict:
    splits = jax.random.split(jax.random.key(seed), 15)
    part_splits = jax.random.split(jax.random.fold_in(splits[14], part), 15)
    return {
        "tokens": gaussian(part_splits[0], (TOKENS, D), 1.0, 6.0, ((0, 16),)),
        "mix_gain": jnp.clip(1.0 + 0.18 * jax.random.normal(splits[1], (D,), jnp.float32), 0.099609375, 1.8984375).astype(jnp.bfloat16),
        "val_weight": draw_val_weight(jax.random.fold_in(splits[14], 71), part),
        "gate_weight": gaussian(splits[3], (D, CH), D ** -0.5, 0.125, ((0, 4), (1, 4))),
        "conv_taps": gaussian(splits[4], (CONV_TAPS, CH), CONV_TAPS ** -0.5, 1.0),
        "chan_gain": jnp.clip(1.0 + 0.18 * jax.random.normal(splits[5], (CH,), jnp.float32), 0.099609375, 1.8984375).astype(jnp.bfloat16),
        "out_weight": gaussian(splits[6], (CH, D), CH ** -0.5, 0.1875, ((0, 4), (1, 4))),
        "mix_post_gain": jnp.clip(1.0 + 0.18 * jax.random.normal(splits[7], (D,), jnp.float32), 0.099609375, 1.8984375).astype(jnp.bfloat16),
        "ffn_gain": jnp.clip(1.0 + 0.18 * jax.random.normal(splits[8], (D,), jnp.float32), 0.099609375, 1.8984375).astype(jnp.bfloat16),
        "up_gate_weight": gaussian(splits[9], (D, FF), D ** -0.5, 0.125, ((0, 4), (1, 4))),
        "up_val_weight": gaussian(splits[10], (D, FF), D ** -0.5, 0.125, ((0, 4), (1, 4))),
        "ffn_taps": gaussian(splits[11], (2, FFN_TAPS, FF), FFN_TAPS ** -0.5, 3.5),
        "down_weight": gaussian(splits[12], (FF, D), FF ** -0.5, 0.078125, ((0, 4), (1, 4))),
        "ffn_post_gain": jnp.clip(1.0 + 0.18 * jax.random.normal(splits[13], (D,), jnp.float32), 0.099609375, 1.8984375).astype(jnp.bfloat16),
    }


norm_epsilon = 1e-06
chan_epsilon = 1e-05

def rms_scale(values, gain):
    inverse = lax.rsqrt(lax.optimization_barrier(jnp.mean(values * values, axis=-1, keepdims=True)) + norm_epsilon)
    return values * inverse * gain.astype(jnp.float32)

def depthwise(signal, tap_table):
    taps_count = tap_table.shape[0]
    channels = signal.shape[1]
    shaped = signal.astype(jnp.float32).reshape(signal.shape[0] // LEN, LEN, channels)
    padded = jnp.pad(shaped, ((0, 0), (taps_count - 1, 0), (0, 0)))
    tap_values = tap_table.astype(jnp.float32)
    result = jnp.zeros(shaped.shape, jnp.float32)
    for offset in range(taps_count):
        result = result + padded[:, offset:offset + LEN, :] * tap_values[offset]
    return result.reshape(signal.shape[0], channels)

def grouped_sum(left, weight):
    group_width = left.shape[1] // N_TP

    def step(running, group_index):
        columns = lax.dynamic_slice_in_dim(left, group_index * group_width, group_width, 1)
        row_block = lax.dynamic_slice_in_dim(weight, group_index * group_width, group_width, 0)
        partial_value = jnp.dot(columns, row_block, preferred_element_type=jnp.float32).astype(jnp.bfloat16)
        partial_value = lax.optimization_barrier(partial_value)
        return (running + partial_value.astype(jnp.float32), None)
    start_sum = jnp.zeros((left.shape[0], weight.shape[1]), jnp.float32)
    running, _ = lax.scan(step, start_sum, jnp.arange(N_TP, dtype=jnp.int32))
    return running

def reference(tokens, mix_gain, val_weight, gate_weight, conv_taps, chan_gain, out_weight, mix_post_gain, ffn_gain, up_gate_weight, up_val_weight, ffn_taps, down_weight, ffn_post_gain):
    normed = rms_scale(tokens.astype(jnp.float32), mix_gain).astype(jnp.bfloat16)
    values = jnp.dot(normed, val_weight, preferred_element_type=jnp.float32)
    gate_sums = jnp.dot(normed, gate_weight, preferred_element_type=jnp.float32)
    glu_out = (values * jax.nn.sigmoid(gate_sums)).astype(jnp.bfloat16)
    conv_out = depthwise(glu_out, conv_taps)
    chan_mean = lax.optimization_barrier(jnp.mean(conv_out, axis=-1, keepdims=True))
    chan_var = lax.optimization_barrier(jnp.mean(conv_out * conv_out, axis=-1, keepdims=True)) - chan_mean * chan_mean
    scaled = (conv_out - chan_mean) * lax.rsqrt(chan_var + chan_epsilon) * chan_gain.astype(jnp.float32)
    activated = jax.nn.silu(scaled).astype(jnp.bfloat16)
    mixed_sum = grouped_sum(activated, out_weight)
    residual = (tokens.astype(jnp.float32) + rms_scale(mixed_sum, mix_post_gain)).astype(jnp.bfloat16)
    normed_ffn = rms_scale(residual.astype(jnp.float32), ffn_gain).astype(jnp.bfloat16)
    up_gate = jnp.dot(normed_ffn, up_gate_weight, preferred_element_type=jnp.float32).astype(jnp.bfloat16)
    up_val = jnp.dot(normed_ffn, up_val_weight, preferred_element_type=jnp.float32).astype(jnp.bfloat16)
    gate_conv = depthwise(up_gate, ffn_taps[0])
    val_conv = depthwise(up_val, ffn_taps[1])
    hidden = (jax.nn.gelu(gate_conv, approximate=True) * val_conv).astype(jnp.bfloat16)
    ffn_sum = grouped_sum(hidden, down_weight)
    return (residual.astype(jnp.float32) + rms_scale(ffn_sum, ffn_post_gain)).astype(jnp.bfloat16)
```

```python
import functools

import jax
import jax.numpy as jnp
from jax import lax
from jax.experimental import pallas as pl
from jax.experimental.pallas import tpu as pltpu
from jax.sharding import PartitionSpec as P

LEN = 64
LANES = 128
F32 = jnp.float32
BF16 = jnp.bfloat16

norm_epsilon = 1e-06
chan_epsilon = 1e-05


def rms_scale(values, gain):
    inverse = lax.rsqrt(jnp.mean(values * values, axis=-1, keepdims=True) + norm_epsilon)
    return values * inverse * gain.astype(F32)


def depthwise(signal, tap_table):
    taps_count = tap_table.shape[0]
    channels = signal.shape[1]
    shaped = signal.astype(F32).reshape(signal.shape[0] // LEN, LEN, channels)
    padded = jnp.pad(shaped, ((0, 0), (taps_count - 1, 0), (0, 0)))
    tap_values = tap_table.astype(F32)
    result = jnp.zeros(shaped.shape, F32)
    for offset in range(taps_count):
        result = result + padded[:, offset : offset + LEN, :] * tap_values[offset]
    return result.reshape(signal.shape[0], channels)


def gather_rows(weight):
    return lax.all_gather(weight, "fs", axis=0, tiled=True)


def gather_columns(weight):
    return lax.all_gather(weight, "fs", axis=1, tiled=True)


def product(left, right):
    return jnp.dot(left, right, preferred_element_type=F32)


def scatter_sum(part):
    return lax.psum_scatter(
        part.astype(BF16), "tp", scatter_dimension=0, tiled=True
    ).astype(F32)


def plain(
    tokens,
    mix_gain,
    val_weight,
    gate_weight,
    conv_taps,
    chan_gain,
    out_weight,
    mix_post_gain,
    ffn_gain,
    up_gate_weight,
    up_val_weight,
    ffn_taps,
    down_weight,
    ffn_post_gain,
):
    member = lax.axis_index("tp")
    normed_own = rms_scale(tokens.astype(F32), mix_gain).astype(BF16)
    normed = lax.all_gather(normed_own, "tp", axis=0, tiled=True)
    local_ch = val_weight.shape[1]
    values = product(normed, gather_rows(val_weight))
    gate_sums = product(normed, gather_rows(gate_weight))
    glu_out = (values * jax.nn.sigmoid(gate_sums)).astype(BF16)
    own_taps = lax.dynamic_slice_in_dim(conv_taps, member * local_ch, local_ch, 1)
    conv_out = depthwise(glu_out, own_taps)
    totals, squares = lax.psum(
        (jnp.sum(conv_out, axis=1), jnp.sum(conv_out * conv_out, axis=1)), "tp"
    )
    all_channels = chan_gain.shape[0]
    chan_mean = totals[:, None] / all_channels
    chan_var = squares[:, None] / all_channels - chan_mean * chan_mean
    own_gain = lax.dynamic_slice_in_dim(chan_gain, member * local_ch, local_ch, 0).astype(F32)
    activated = jax.nn.silu((conv_out - chan_mean) * lax.rsqrt(chan_var + chan_epsilon) * own_gain)
    mixed_sum = scatter_sum(product(activated.astype(BF16), gather_columns(out_weight)))
    residual = (tokens.astype(F32) + rms_scale(mixed_sum, mix_post_gain)).astype(BF16)
    normed_share = rms_scale(residual.astype(F32), ffn_gain).astype(BF16)
    normed_ffn = lax.all_gather(normed_share, "tp", axis=0, tiled=True)
    local_ff = up_gate_weight.shape[1]
    own_ffn_taps = lax.dynamic_slice_in_dim(ffn_taps, member * local_ff, local_ff, 2)
    up_gate = product(normed_ffn, gather_rows(up_gate_weight)).astype(BF16)
    up_val = product(normed_ffn, gather_rows(up_val_weight)).astype(BF16)
    gate_conv = depthwise(up_gate, own_ffn_taps[0])
    val_conv = depthwise(up_val, own_ffn_taps[1])
    hidden = (jax.nn.gelu(gate_conv, approximate=True) * val_conv).astype(BF16)
    ffn_sum = scatter_sum(product(hidden, gather_columns(down_weight)))
    return (residual.astype(F32) + rms_scale(ffn_sum, ffn_post_gain)).astype(BF16)


def rows_at(start, size, unit=16):
    return pl.ds(pl.multiple_of(start, unit), size)


class Where:
    def __init__(self):
        self.place = lax.axis_index("fs")
        self.half = lax.axis_index("grp")
        self.member = lax.axis_index("tp")
        place, member = self.place, self.member
        self.side = place // 2
        self.inner = jnp.logical_or(place == 1, place == 2)
        self.chip = member // 2
        self.core = member % 2
        self.mate = place + 1 - 2 * (place % 2)
        self.over = 2 - self.side
        self.pair = lax.rem(place + 2, 4)
        self.sibling = member + 1 - 2 * self.core
        self.across = lax.rem(member + 2, 4)
        self.corner = self.sibling + 2 - 4 * self.chip

    def source(self, slot):
        if slot == 1:
            return self.mate
        if slot == 2:
            return self.pair
        return self.pair + 1 - 2 * (self.place % 2)


class Piece:
    def __init__(self, source, held, start, size, stride, sided, columns):
        self.source_ref = source
        self.held = held
        self.start = start
        self.size = size
        self.stride = stride
        self.sided = sided
        self.columns = columns

    def read(self, where, side):
        first = where.half * self.stride + self.start
        if self.sided == "rows":
            first = side * (2 * self.stride) + first
        rows = rows_at(first, self.size)
        if self.sided == "columns":
            columns = rows_at(side * self.columns, self.columns, LANES)
            return self.source_ref.at[rows, columns]
        return self.source_ref.at[rows]

    def target(self, where, origin, half):
        first = half * self.stride + self.start
        return self.held.at[origin, rows_at(first, self.size)]


class Stream:
    def __init__(self, where, pieces, semaphores):
        self.where = where
        self.pieces = pieces
        self.z_send, self.z_recv, self.y_send, self.y_recv = semaphores

    def z_copy(self, unit, kind):
        w, piece = self.where, self.pieces[unit]
        if kind < 2:
            side = w.side if kind == 0 else 1 - w.side
            source = piece.read(w, side)
            target = piece.target(w, w.place, w.half)
            device = w.mate if kind == 0 else w.over
            if kind == 0:
                slot = 1
            else:
                slot = 2 + w.inner.astype(jnp.int32)
        else:
            target = piece.target(w, w.source(kind), w.half)
            source = target
            device = w.mate
            slot = 5 - kind
        return pltpu.make_async_remote_copy(
            src_ref=source,
            dst_ref=target,
            send_sem=self.z_send.at[unit, kind],
            recv_sem=self.z_recv.at[unit, slot - 1],
            device_id={"fs": device},
        )

    def z_arrival(self, unit, slot):
        w = self.where
        target = self.pieces[unit].target(w, w.source(slot), w.half)
        return pltpu.make_async_remote_copy(
            src_ref=target,
            dst_ref=target,
            send_sem=self.z_send.at[unit, 0],
            recv_sem=self.z_recv.at[unit, slot - 1],
            device_id={"fs": w.mate},
        )

    def y_copy(self, unit, slot, incoming=False):
        w = self.where
        half = 1 - w.half if incoming else w.half
        target = self.pieces[unit].target(w, w.source(slot), half)
        return pltpu.make_async_remote_copy(
            src_ref=target,
            dst_ref=target,
            send_sem=self.y_send.at[unit, slot - 1],
            recv_sem=self.y_recv.at[unit, slot - 1],
            device_id={"grp": 1 - w.half},
        )

    def start(self, unit):
        self.z_copy(unit, 0).start()
        self.z_copy(unit, 1).start()

    def serve(self, unit, slot):
        self.z_arrival(unit, slot).wait_recv()
        if slot > 1:

            @pl.when(self.where.inner)
            def _():
                self.z_copy(unit, slot).start()

        self.y_copy(unit, slot).start()

    def serve_unit(self, unit):
        for slot in (1, 3, 2):
            self.serve(unit, slot)

    def arrive(self, unit):
        for slot in (1, 3, 2):
            self.y_copy(unit, slot, incoming=True).wait_recv()

    def drain(self, unit):
        self.z_copy(unit, 0).wait_send()
        self.z_copy(unit, 1).wait_send()
        for slot in (1, 2, 3):
            if slot > 1:

                @pl.when(self.where.inner)
                def _():
                    self.z_copy(unit, slot).wait_send()

            self.y_copy(unit, slot).wait_send()


class RowGather:
    def __init__(self, where, held, rows, group_rows, semaphores):
        self.where = where
        self.held = held
        self.rows = rows
        self.group_rows = group_rows
        self.send, self.recv = semaphores

    def view(self, level, member):
        first = level * self.group_rows + member * self.rows
        return self.held.at[rows_at(first, self.rows)]

    def copy(self, level, kind):
        w = self.where
        view = self.view(level, w.across if kind == 2 else w.member)
        return pltpu.make_async_remote_copy(
            src_ref=view,
            dst_ref=view,
            send_sem=self.send.at[level, kind],
            recv_sem=self.recv.at[level, kind],
            device_id={"tp": w.across if kind == 1 else w.sibling},
        )

    def arrival(self, level, kind):
        w = self.where
        member = (w.sibling, w.across, w.corner)[kind]
        view = self.view(level, member)
        return pltpu.make_async_remote_copy(
            src_ref=view,
            dst_ref=view,
            send_sem=self.send.at[level, kind],
            recv_sem=self.recv.at[level, kind],
            device_id={"tp": w.across if kind == 1 else w.sibling},
        )

    def start(self, level):
        self.copy(level, 1).start()
        self.copy(level, 0).start()

    def relay(self, level):
        self.arrival(level, 1).wait_recv()
        self.copy(level, 2).start()

    def finish(self, level):
        self.arrival(level, 0).wait_recv()
        self.arrival(level, 2).wait_recv()

    def drain(self, level):
        for kind in range(3):
            self.copy(level, kind).wait_send()

    def pair_copy(self, incoming=False):
        w = self.where
        mine = self.view(0, w.member)
        other = self.view(1, w.member)
        return pltpu.make_async_remote_copy(
            src_ref=other if incoming else mine,
            dst_ref=other,
            send_sem=self.send.at[1, 3],
            recv_sem=self.recv.at[1, 3],
            device_id={"fs": w.pair},
        )


class RowScatter:
    def __init__(self, where, levels, rows, width, part, sends, recvs, semaphores, result):
        self.where = where
        self.levels = levels
        self.rows = rows
        self.width = width
        self.part = part
        self.sends = sends
        self.recvs = recvs
        self.send_sem, self.recv_sem = semaphores
        self.result = result

    def copy(self, block, stage):
        w = self.where
        device = ({"tp": w.sibling}, {"tp": w.across}, {"fs": w.pair})[stage]
        return pltpu.make_async_remote_copy(
            src_ref=self.sends[stage].at[block],
            dst_ref=self.recvs[stage].at[block],
            send_sem=self.send_sem.at[stage, block],
            recv_sem=self.recv_sem.at[stage, block],
            device_id=device,
        )

    def begin(self, block, value):
        w = self.where
        shape = (self.levels, 2, 2, self.rows, self.width)
        self.part[block] = value.reshape(shape)
        self.sends[0][block] = self.part[block, :, :, 1 - w.core].astype(BF16)
        self.copy(block, 0).start()

    def second(self, block):
        w = self.where
        self.copy(block, 0).wait_recv()
        away = self.part[block, :, 1 - w.chip, w.core]
        away = away + self.recvs[0][block, :, 1 - w.chip].astype(F32)
        self.sends[1][block] = away.astype(BF16)
        self.copy(block, 1).start()
        kept = self.part[block, :, w.chip, w.core]
        kept = kept + self.recvs[0][block, :, w.chip].astype(F32)
        self.part[block, :, 0, 0] = kept

    def third(self, block):
        self.copy(block, 1).wait_recv()
        if self.levels > 1:
            away = self.part[block, 1, 0, 0] + self.recvs[1][block, 1].astype(F32)
            self.sends[2][block] = away.astype(BF16)
            self.copy(block, 2).start()
            kept = self.part[block, 0, 0, 0] + self.recvs[1][block, 0].astype(F32)
            self.part[block, 0, 0, 0] = kept
        else:
            self.store(block, self.part[block, 0, 0, 0] + self.recvs[1][block, 0].astype(F32))

    def fourth(self, block):
        self.copy(block, 2).wait_recv()
        self.store(block, self.part[block, 0, 0, 0] + self.recvs[2][block].astype(F32))

    def store(self, block, value):
        self.result[:, rows_at(block * self.width, self.width, LANES)] = value

    def drain(self, block):
        for stage in range(1 + self.levels):
            self.copy(block, stage).wait_send()


def layer_kernel(sizes, *refs):
    (
        tokens,
        mix_gain,
        val_weight,
        gate_weight,
        conv_taps,
        chan_gain,
        out_weight,
        mix_post_gain,
        ffn_gain,
        up_gate_weight,
        up_val_weight,
        ffn_taps,
        down_weight,
        ffn_post_gain,
        layer_out,
        val_all,
        gate_all,
        out_all,
        up_gate_all,
        up_val_all,
        down_all,
        mix_rows,
        ffn_rows,
        glu_padded,
        conv_out,
        stats,
        activated,
        up_padded,
        hidden,
        residual_ref,
        result,
        mix_part,
        ffn_part,
        mix_send0,
        mix_send1,
        mix_recv0,
        mix_recv1,
        ffn_send0,
        ffn_send1,
        ffn_send2,
        ffn_recv0,
        ffn_recv1,
        ffn_recv2,
        own_sem,
        z_send,
        z_recv,
        y_send,
        y_recv,
        mix_row_send,
        mix_row_recv,
        ffn_row_send,
        ffn_row_recv,
        stat_send,
        stat_recv,
        mix_sum_send,
        mix_sum_recv,
        ffn_sum_send,
        ffn_sum_recv,
    ) = refs
    w = Where()
    rows, group_rows, segments = sizes["rows"], sizes["group_rows"], sizes["segments"]
    depth, local_ch, half_ff = sizes["depth"], sizes["local_ch"], sizes["half_ff"]
    width = out_all.shape[2]
    mix_tiles, ffn_tiles = local_ch // LANES, half_ff // LANES
    member = w.member

    barrier = pltpu.get_barrier_semaphore()
    friends = [
        {"tp": w.sibling},
        {"tp": w.across},
        {"tp": w.corner},
        {"grp": 1 - w.half},
        {"fs": w.mate},
        {"fs": w.pair},
    ]
    for friend in friends:
        pl.semaphore_signal(barrier, inc=1, device_id=friend)

    @pl.when(w.inner)
    def _():
        pl.semaphore_signal(barrier, inc=1, device_id={"fs": 3 - w.place})

    pieces = []

    def cut(source, held, sided, chunks):
        total = held.shape[1] // 2
        size = total // chunks
        return [
            Piece(source, held, index * size, size, total, sided, held.shape[2])
            for index in range(chunks)
        ]

    val_pieces = cut(val_weight, val_all, None, 2)
    gate_pieces = cut(gate_weight, gate_all, None, 2)
    out_pieces = cut(out_weight, out_all, None, 2)
    up_gate_pieces = cut(up_gate_weight, up_gate_all, "columns", 2)
    up_val_pieces = cut(up_val_weight, up_val_all, "columns", 2)
    down_pieces = cut(down_weight, down_all, "rows", sizes["down_chunks"])
    first = [val_pieces[0], gate_pieces[0], val_pieces[1], gate_pieces[1]]
    later = [up_gate_pieces[0], up_val_pieces[0], up_gate_pieces[1], up_val_pieces[1]]
    pieces = first + out_pieces + later + down_pieces
    proj = list(range(0, 4))
    outs = list(range(4, 6))
    ups = list(range(6, 10))
    downs = list(range(10, 10 + len(down_pieces)))
    stream = Stream(w, pieces, (z_send, z_recv, y_send, y_recv))

    def own_copy(index, source, held, sided):
        if sided == "columns":
            view = source.at[:, rows_at(w.side * held.shape[2], held.shape[2], LANES)]
        elif sided == "rows":
            view = source.at[rows_at(w.side * held.shape[1], held.shape[1])]
        else:
            view = source
        return pltpu.make_async_copy(view, held.at[w.place], own_sem.at[index])

    own_copies = [
        own_copy(0, val_weight, val_all, None),
        own_copy(1, gate_weight, gate_all, None),
        own_copy(2, out_weight, out_all, None),
        own_copy(3, up_gate_weight, up_gate_all, "columns"),
        own_copy(4, up_val_weight, up_val_all, "columns"),
        own_copy(5, down_weight, down_all, "rows"),
    ]
    for copy in own_copies:
        copy.start()

    glu_padded[:, 0:32, :] = jnp.zeros((glu_padded.shape[0], 32, LANES), F32)
    up_padded[:, :, 0:8, :] = jnp.zeros((2, up_padded.shape[1], 8, LANES), F32)
    own_rows = rows_at(member * rows, rows)
    mix_rows[own_rows] = rms_scale(tokens[...].astype(F32), mix_gain[...]).astype(BF16)

    pl.semaphore_wait(barrier, len(friends) + w.inner.astype(jnp.int32))

    for unit in proj + outs:
        stream.start(unit)
    mix_gather = RowGather(w, mix_rows, rows, group_rows, (mix_row_send, mix_row_recv))
    mix_gather.start(0)
    stream.serve_unit(0)
    stream.serve_unit(1)
    mix_gather.relay(0)
    stream.serve_unit(2)
    stream.serve_unit(3)
    stream.serve_unit(4)
    for unit in ups[:2]:
        stream.start(unit)
    for unit in proj:
        stream.arrive(unit)
    own_copies[0].wait()
    own_copies[1].wait()
    mix_gather.finish(0)

    left = mix_rows[...]
    values = product(left, val_all[...].reshape(depth, local_ch))
    gate_sums = product(left, gate_all[...].reshape(depth, local_ch))
    glu = (values * jax.nn.sigmoid(gate_sums)).astype(BF16).astype(F32)
    for tile in range(mix_tiles):
        block = glu[:, tile * LANES : (tile + 1) * LANES].reshape(segments, LEN, LANES)
        glu_padded[tile * segments : (tile + 1) * segments, 32:, :] = block
    stream.serve_unit(5)
    for unit in ups[2:]:
        stream.start(unit)

    taps_count = conv_taps.shape[0]
    for tile in range(mix_tiles):
        lanes = rows_at(member * local_ch + tile * LANES, LANES, LANES)
        taps = conv_taps[:, lanes].astype(F32)

        @pl.loop(0, segments)
        def _(segment):
            total = jnp.zeros((LEN, LANES), F32)
            for k in range(taps_count):
                shifted = glu_padded[tile * segments + segment, pl.ds(33 - taps_count + k, LEN), :]
                total = total + shifted * taps[k : k + 1]
            conv_out[tile, rows_at(segment * LEN, LEN)] = total

    sums = conv_out[0]
    squares = conv_out[0] * conv_out[0]
    for tile in range(1, mix_tiles):
        sums = sums + conv_out[tile]
        squares = squares + conv_out[tile] * conv_out[tile]
    exact = lax.Precision.HIGHEST
    ones = jnp.ones((8, LANES), F32)
    contract_lanes = (((1,), (1,)), ((), ()))
    sums = lax.dot_general(ones, sums, contract_lanes, precision=exact, preferred_element_type=F32)
    squares = lax.dot_general(
        ones, squares, contract_lanes, precision=exact, preferred_element_type=F32
    )
    upper = lax.broadcasted_iota(jnp.int32, (8, group_rows), 0) < 4
    stats[0, :, :] = jnp.zeros(stats.shape[1:], F32)
    stats[0, :, 0:group_rows] = jnp.where(upper, sums, squares)

    def stat_copy(kind):
        device = (w.sibling, w.across, w.corner)[kind]
        return pltpu.make_async_remote_copy(
            src_ref=stats.at[0],
            dst_ref=stats.at[1 + kind],
            send_sem=stat_send.at[kind],
            recv_sem=stat_recv.at[kind],
            device_id={"tp": device},
        )

    for kind in (2, 1, 0):
        stat_copy(kind).start()
    stream.serve_unit(6)
    for unit in outs:
        stream.arrive(unit)
    own_copies[2].wait()
    for kind in range(3):
        stat_copy(kind).wait_recv()
    total = stats[0] + stats[1] + stats[2] + stats[3]
    flipped = jnp.transpose(total)[:group_rows] / chan_gain.shape[1]
    chan_mean = flipped[:, 0:1]
    chan_var = flipped[:, 4:5] - chan_mean * chan_mean
    inverse = lax.rsqrt(chan_var + chan_epsilon)
    for tile in range(mix_tiles):
        lanes = rows_at(member * local_ch + tile * LANES, LANES, LANES)
        scaled = (conv_out[tile] - chan_mean) * inverse * chan_gain[:, lanes].astype(F32)
        activated[:, tile * LANES : (tile + 1) * LANES] = jax.nn.silu(scaled).astype(BF16)

    mix_sum = RowScatter(
        w,
        1,
        rows,
        width,
        mix_part,
        (mix_send0, mix_send1),
        (mix_recv0, mix_recv1),
        (mix_sum_send, mix_sum_recv),
        result,
    )
    places = [w.place, w.mate, w.source(3), w.source(2)]
    for index in range(4 + 2):
        if index < 4:
            block = places[index]
            mix_sum.begin(block, product(activated[...], out_all[block]))
        if 1 <= index < 5:
            mix_sum.second(places[index - 1])
        if 2 <= index:
            mix_sum.third(places[index - 2])

    residual = tokens[...].astype(F32) + rms_scale(result[...], mix_post_gain[...])
    residual = residual.astype(BF16)
    residual_ref[...] = residual
    ffn_rows[own_rows] = rms_scale(residual.astype(F32), ffn_gain[...]).astype(BF16)
    ffn_gather = RowGather(w, ffn_rows, rows, group_rows, (ffn_row_send, ffn_row_recv))
    ffn_gather.start(0)
    ffn_gather.pair_copy().start()
    for unit in downs[:2]:
        stream.start(unit)
    stream.serve_unit(7)
    ffn_gather.relay(0)
    stream.serve_unit(8)
    ffn_gather.pair_copy(incoming=True).wait_recv()
    ffn_gather.start(1)
    stream.serve_unit(9)
    for unit in downs[2:]:
        stream.start(unit)
    ffn_gather.relay(1)
    stream.serve_unit(downs[0])
    for unit in ups:
        stream.arrive(unit)
    own_copies[3].wait()
    own_copies[4].wait()

    def feed(level):
        ffn_gather.finish(level)
        left = ffn_rows[level * group_rows : (level + 1) * group_rows]
        for half, weight in enumerate((up_gate_all, up_val_all)):
            up = product(left, weight[...].reshape(depth, half_ff)).astype(BF16).astype(F32)
            for tile in range(ffn_tiles):
                block = up[:, tile * LANES : (tile + 1) * LANES].reshape(segments, LEN, LANES)
                up_padded[half, tile * segments : (tile + 1) * segments, 8:, :] = block
        for tile in range(ffn_tiles):
            first_lane = (2 * member + w.side) * half_ff + tile * LANES
            lanes = rows_at(first_lane, LANES, LANES)
            taps = [ffn_taps[half, :, lanes].astype(F32) for half in range(2)]

            @pl.loop(0, segments)
            def _(segment):
                convs = []
                for half in range(2):
                    conv = jnp.zeros((LEN, LANES), F32)
                    count = ffn_taps.shape[1]
                    for k in range(count):
                        shifted = up_padded[
                            half, tile * segments + segment, pl.ds(9 - count + k, LEN), :
                        ]
                        conv = conv + shifted * taps[half][k : k + 1]
                    convs.append(conv)
                value = jax.nn.gelu(convs[0], approximate=True) * convs[1]
                at = rows_at(level * group_rows + segment * LEN, LEN)
                hidden[at, tile * LANES : (tile + 1) * LANES] = value.astype(BF16)

    feed(0)
    stream.serve_unit(downs[1])
    feed(1)
    for unit in downs[2:]:
        stream.serve_unit(unit)
    ffn_sum = RowScatter(
        w,
        2,
        rows,
        width,
        ffn_part,
        (ffn_send0, ffn_send1, ffn_send2),
        (ffn_recv0, ffn_recv1, ffn_recv2),
        (ffn_sum_send, ffn_sum_recv),
        result,
    )
    own_copies[5].wait()
    slots = [None, 1, 3, 2]
    for index in range(4 + 2):
        if index < 4:
            block = places[index]
            if index > 0:
                for unit in downs:
                    stream.y_copy(unit, slots[index], incoming=True).wait_recv()
            ffn_sum.begin(block, product(hidden[...], down_all[block]))
        if 1 <= index < 5:
            ffn_sum.second(places[index - 1])
        if 2 <= index:
            ffn_sum.third(places[index - 2])
    for index in (3, 2, 1, 0):
        ffn_sum.fourth(places[3 - index])
    final = residual_ref[...].astype(F32) + rms_scale(result[...], ffn_post_gain[...])
    layer_out[...] = final.astype(BF16)

    for unit in range(len(pieces)):
        stream.drain(unit)
    mix_gather.drain(0)
    ffn_gather.drain(0)
    ffn_gather.drain(1)
    ffn_gather.pair_copy().wait_send()
    for kind in range(3):
        stat_copy(kind).wait_send()
    for index in range(4):
        mix_sum.drain(places[index])
        ffn_sum.drain(places[index])


def kernel_sizes(tokens, val_weight, out_weight, up_gate_weight, down_weight):
    rows = tokens.shape[0]
    return {
        "rows": rows,
        "group_rows": 4 * rows,
        "segments": 4 * rows // LEN,
        "depth": 4 * val_weight.shape[0],
        "local_ch": val_weight.shape[1],
        "half_ff": up_gate_weight.shape[1] // 2,
        "down_chunks": 4,
    }


def run_kernel(*args):
    (
        tokens,
        mix_gain,
        val_weight,
        gate_weight,
        conv_taps,
        chan_gain,
        out_weight,
        mix_post_gain,
        ffn_gain,
        up_gate_weight,
        up_val_weight,
        ffn_taps,
        down_weight,
        ffn_post_gain,
    ) = args
    sizes = kernel_sizes(tokens, val_weight, out_weight, up_gate_weight, down_weight)
    rows, group_rows, segments = sizes["rows"], sizes["group_rows"], sizes["segments"]
    local_ch, half_ff = sizes["local_ch"], sizes["half_ff"]
    width = out_weight.shape[1]
    model = tokens.shape[1]
    mix_tiles, ffn_tiles = local_ch // LANES, half_ff // LANES
    padded_rows = -(-group_rows // LANES) * LANES
    units = 10 + sizes["down_chunks"]
    dma = pltpu.SemaphoreType.DMA
    vmem, anywhere = pl.BlockSpec(memory_space=pltpu.VMEM), pl.BlockSpec(memory_space=pl.ANY)
    shaped = [
        tokens,
        mix_gain[None],
        val_weight,
        gate_weight,
        conv_taps,
        chan_gain[None],
        out_weight,
        mix_post_gain[None],
        ffn_gain[None],
        up_gate_weight,
        up_val_weight,
        ffn_taps,
        down_weight,
        ffn_post_gain[None],
    ]
    weights = (2, 3, 6, 9, 10, 12)
    scratch = [
        pltpu.VMEM((4, val_weight.shape[0], local_ch), BF16),
        pltpu.VMEM((4, gate_weight.shape[0], local_ch), BF16),
        pltpu.VMEM((4, local_ch, width), BF16),
        pltpu.VMEM((4, up_gate_weight.shape[0], half_ff), BF16),
        pltpu.VMEM((4, up_val_weight.shape[0], half_ff), BF16),
        pltpu.VMEM((4, half_ff, width), BF16),
        pltpu.VMEM((group_rows, model), BF16),
        pltpu.VMEM((2 * group_rows, model), BF16),
        pltpu.VMEM((mix_tiles * segments, 32 + LEN, LANES), F32),
        pltpu.VMEM((mix_tiles, group_rows, LANES), F32),
        pltpu.VMEM((4, 8, padded_rows), F32),
        pltpu.VMEM((group_rows, local_ch), BF16),
        pltpu.VMEM((2, ffn_tiles * segments, 8 + LEN, LANES), F32),
        pltpu.VMEM((2 * group_rows, half_ff), BF16),
        pltpu.VMEM((rows, model), BF16),
        pltpu.VMEM((rows, model), F32),
        pltpu.VMEM((4, 1, 2, 2, rows, width), F32),
        pltpu.VMEM((4, 2, 2, 2, rows, width), F32),
        pltpu.VMEM((4, 1, 2, rows, width), BF16),
        pltpu.VMEM((4, 1, rows, width), BF16),
        pltpu.VMEM((4, 1, 2, rows, width), BF16),
        pltpu.VMEM((4, 1, rows, width), BF16),
        pltpu.VMEM((4, 2, 2, rows, width), BF16),
        pltpu.VMEM((4, 2, rows, width), BF16),
        pltpu.VMEM((4, rows, width), BF16),
        pltpu.VMEM((4, 2, 2, rows, width), BF16),
        pltpu.VMEM((4, 2, rows, width), BF16),
        pltpu.VMEM((4, rows, width), BF16),
        dma((6,)),
        dma((units, 4)),
        dma((units, 3)),
        dma((units, 3)),
        dma((units, 3)),
        dma((1, 3)),
        dma((1, 3)),
        dma((2, 4)),
        dma((2, 4)),
        dma((3,)),
        dma((3,)),
        dma((2, 4)),
        dma((2, 4)),
        dma((3, 4)),
        dma((3, 4)),
    ]
    return pl.pallas_call(
        functools.partial(layer_kernel, sizes),
        out_shape=jax.ShapeDtypeStruct(tokens.shape, BF16),
        in_specs=[anywhere if index in weights else vmem for index in range(len(shaped))],
        out_specs=vmem,
        scratch_shapes=scratch,
        compiler_params=pltpu.CompilerParams(
            collective_id=0, has_side_effects=True, vmem_limit_bytes=56_000_000
        ),
    )(*shaped)


def fits(mesh, args):
    tokens, val_weight, out_weight = args[0], args[2], args[6]
    up_gate_weight, down_weight = args[9], args[12]
    if (mesh.shape["grp"], mesh.shape["fs"], mesh.shape["tp"]) != (2, 4, 4):
        return False
    rows = tokens.shape[0] // 32
    local_ch, local_ff = val_weight.shape[1] // 4, up_gate_weight.shape[1] // 4
    local_model = tokens.shape[1] // 4
    return (
        rows % 16 == 0
        and 4 * rows % LEN == 0
        and local_ch % LANES == 0
        and local_ff % (2 * LANES) == 0
        and local_model % LANES == 0
        and args[4].shape[0] <= 32
        and args[11].shape[1] <= 8
    )


def solution(mesh):
    specs = (
        P(("grp", "fs", "tp"), None),
        P(),
        P("fs", "tp"),
        P("fs", "tp"),
        P(),
        P(),
        P("tp", "fs"),
        P(),
        P(),
        P("fs", "tp"),
        P("fs", "tp"),
        P(),
        P("tp", "fs"),
        P(),
    )

    def whole(*args):
        body = run_kernel if fits(mesh, args) else plain
        step = jax.shard_map(
            body,
            mesh=mesh,
            in_specs=specs,
            out_specs=P(("grp", "fs", "tp"), None),
            check_vma=False,
        )
        return step(*args)

    return whole
```

```python
import functools

import jax
import jax.numpy as jnp
from jax import lax
from jax.experimental import pallas as pl
from jax.experimental.pallas import tpu as pltpu
from jax.sharding import PartitionSpec as P

LEN = 64
LANES = 128
F32 = jnp.float32
BF16 = jnp.bfloat16

norm_epsilon = 1e-06
chan_epsilon = 1e-05


def rms_scale(values, gain):
    inverse = lax.rsqrt(jnp.mean(values * values, axis=-1, keepdims=True) + norm_epsilon)
    return values * inverse * gain.astype(F32)


def depthwise(signal, tap_table):
    taps_count = tap_table.shape[0]
    channels = signal.shape[1]
    shaped = signal.astype(F32).reshape(signal.shape[0] // LEN, LEN, channels)
    padded = jnp.pad(shaped, ((0, 0), (taps_count - 1, 0), (0, 0)))
    tap_values = tap_table.astype(F32)
    result = jnp.zeros(shaped.shape, F32)
    for offset in range(taps_count):
        result = result + padded[:, offset : offset + LEN, :] * tap_values[offset]
    return result.reshape(signal.shape[0], channels)


def gather_rows(weight):
    return lax.all_gather(weight, "fs", axis=0, tiled=True)


def gather_columns(weight):
    return lax.all_gather(weight, "fs", axis=1, tiled=True)


def product(left, right):
    return jnp.dot(left, right, preferred_element_type=F32)


def scatter_sum(part):
    return lax.psum_scatter(
        part.astype(BF16), "tp", scatter_dimension=0, tiled=True
    ).astype(F32)


def plain(
    tokens,
    mix_gain,
    val_weight,
    gate_weight,
    conv_taps,
    chan_gain,
    out_weight,
    mix_post_gain,
    ffn_gain,
    up_gate_weight,
    up_val_weight,
    ffn_taps,
    down_weight,
    ffn_post_gain,
):
    member = lax.axis_index("tp")
    normed_own = rms_scale(tokens.astype(F32), mix_gain).astype(BF16)
    normed = lax.all_gather(normed_own, "tp", axis=0, tiled=True)
    local_ch = val_weight.shape[1]
    values = product(normed, gather_rows(val_weight))
    gate_sums = product(normed, gather_rows(gate_weight))
    glu_out = (values * jax.nn.sigmoid(gate_sums)).astype(BF16)
    own_taps = lax.dynamic_slice_in_dim(conv_taps, member * local_ch, local_ch, 1)
    conv_out = depthwise(glu_out, own_taps)
    totals, squares = lax.psum(
        (jnp.sum(conv_out, axis=1), jnp.sum(conv_out * conv_out, axis=1)), "tp"
    )
    all_channels = chan_gain.shape[0]
    chan_mean = totals[:, None] / all_channels
    chan_var = squares[:, None] / all_channels - chan_mean * chan_mean
    own_gain = lax.dynamic_slice_in_dim(chan_gain, member * local_ch, local_ch, 0).astype(F32)
    activated = jax.nn.silu((conv_out - chan_mean) * lax.rsqrt(chan_var + chan_epsilon) * own_gain)
    mixed_sum = scatter_sum(product(activated.astype(BF16), gather_columns(out_weight)))
    residual = (tokens.astype(F32) + rms_scale(mixed_sum, mix_post_gain)).astype(BF16)
    normed_share = rms_scale(residual.astype(F32), ffn_gain).astype(BF16)
    normed_ffn = lax.all_gather(normed_share, "tp", axis=0, tiled=True)
    local_ff = up_gate_weight.shape[1]
    own_ffn_taps = lax.dynamic_slice_in_dim(ffn_taps, member * local_ff, local_ff, 2)
    up_gate = product(normed_ffn, gather_rows(up_gate_weight)).astype(BF16)
    up_val = product(normed_ffn, gather_rows(up_val_weight)).astype(BF16)
    gate_conv = depthwise(up_gate, own_ffn_taps[0])
    val_conv = depthwise(up_val, own_ffn_taps[1])
    hidden = (jax.nn.gelu(gate_conv, approximate=True) * val_conv).astype(BF16)
    ffn_sum = scatter_sum(product(hidden, gather_columns(down_weight)))
    return (residual.astype(F32) + rms_scale(ffn_sum, ffn_post_gain)).astype(BF16)


def rows_at(start, size, unit=16):
    return pl.ds(pl.multiple_of(start, unit), size)


class Where:
    def __init__(self):
        self.place = lax.axis_index("fs")
        self.half = lax.axis_index("grp")
        self.member = lax.axis_index("tp")
        place, member = self.place, self.member
        self.side = place // 2
        self.inner = jnp.logical_or(place == 1, place == 2)
        self.chip = member // 2
        self.core = member % 2
        self.mate = place + 1 - 2 * (place % 2)
        self.over = 2 - self.side
        self.pair = lax.rem(place + 2, 4)
        self.sibling = member + 1 - 2 * self.core
        self.across = lax.rem(member + 2, 4)
        self.corner = self.sibling + 2 - 4 * self.chip

    def source(self, slot):
        if slot == 1:
            return self.mate
        if slot == 2:
            return self.pair
        return self.pair + 1 - 2 * (self.place % 2)


class Piece:
    def __init__(self, source, held, start, size, stride, sided, columns):
        self.source_ref = source
        self.held = held
        self.start = start
        self.size = size
        self.stride = stride
        self.sided = sided
        self.columns = columns

    def read(self, where, side):
        first = where.half * self.stride + self.start
        if self.sided == "rows":
            first = side * (2 * self.stride) + first
        rows = rows_at(first, self.size)
        if self.sided == "columns":
            columns = rows_at(side * self.columns, self.columns, LANES)
            return self.source_ref.at[rows, columns]
        return self.source_ref.at[rows]

    def target(self, where, origin, half):
        first = half * self.stride + self.start
        return self.held.at[origin, rows_at(first, self.size)]


class Stream:
    def __init__(self, where, pieces, semaphores):
        self.where = where
        self.pieces = pieces
        self.z_send, self.z_recv, self.y_send, self.y_recv = semaphores

    def z_copy(self, unit, kind):
        w, piece = self.where, self.pieces[unit]
        if kind < 2:
            side = w.side if kind == 0 else 1 - w.side
            source = piece.read(w, side)
            target = piece.target(w, w.place, w.half)
            device = w.mate if kind == 0 else w.over
            if kind == 0:
                slot = 1
            else:
                slot = 2 + w.inner.astype(jnp.int32)
        else:
            target = piece.target(w, w.source(kind), w.half)
            source = target
            device = w.mate
            slot = 5 - kind
        return pltpu.make_async_remote_copy(
            src_ref=source,
            dst_ref=target,
            send_sem=self.z_send.at[unit, kind],
            recv_sem=self.z_recv.at[unit, slot - 1],
            device_id={"fs": device},
        )

    def z_arrival(self, unit, slot):
        w = self.where
        target = self.pieces[unit].target(w, w.source(slot), w.half)
        return pltpu.make_async_remote_copy(
            src_ref=target,
            dst_ref=target,
            send_sem=self.z_send.at[unit, 0],
            recv_sem=self.z_recv.at[unit, slot - 1],
            device_id={"fs": w.mate},
        )

    def y_copy(self, unit, slot, incoming=False):
        w = self.where
        half = 1 - w.half if incoming else w.half
        target = self.pieces[unit].target(w, w.source(slot), half)
        return pltpu.make_async_remote_copy(
            src_ref=target,
            dst_ref=target,
            send_sem=self.y_send.at[unit, slot - 1],
            recv_sem=self.y_recv.at[unit, slot - 1],
            device_id={"grp": 1 - w.half},
        )

    def start(self, unit):
        self.z_copy(unit, 0).start()
        self.z_copy(unit, 1).start()

    def serve(self, unit, slot, relay):
        self.z_arrival(unit, slot).wait_recv()
        if relay:
            self.z_copy(unit, slot).start()
        self.y_copy(unit, slot).start()

    def events(self, order, ahead, lag):
        count = len(order)
        inner, outer = [], []
        for index in range(count + lag):
            first = [order[index + ahead]] if index + ahead < count else []
            for slot in (2, 3, 1):
                if index < count:
                    begin = first if slot == 2 else []
                    inner.append((begin, order[index], slot, slot > 1))
            if index < count:
                outer.append((first, order[index], 1, False))
            if index >= lag:
                outer.append(([], order[index - lag], 3, False))
                outer.append(([], order[index - lag], 2, False))
        self.waiting = list(zip(inner, outer))

    def pump(self, count):
        for _ in range(min(count, len(self.waiting))):
            pair = self.waiting.pop(0)
            for role, (begin, unit, slot, relay) in enumerate(pair):
                chosen = jnp.logical_not(self.where.inner) if role else self.where.inner

                @pl.when(chosen)
                def _():
                    for other in begin:
                        self.start(other)
                    self.serve(unit, slot, relay)

    def arrive(self, unit):
        for slot in (1, 3, 2):
            self.y_copy(unit, slot, incoming=True).wait_recv()

    def drain(self, unit):
        self.z_copy(unit, 0).wait_send()
        self.z_copy(unit, 1).wait_send()
        for slot in (1, 2, 3):
            if slot > 1:

                @pl.when(self.where.inner)
                def _():
                    self.z_copy(unit, slot).wait_send()

            self.y_copy(unit, slot).wait_send()


class RowGather:
    def __init__(self, where, held, rows, group_rows, semaphores):
        self.where = where
        self.held = held
        self.rows = rows
        self.group_rows = group_rows
        self.send, self.recv = semaphores

    def view(self, level, member):
        first = level * self.group_rows + member * self.rows
        return self.held.at[rows_at(first, self.rows)]

    def copy(self, level, kind):
        w = self.where
        view = self.view(level, w.across if kind == 2 else w.member)
        return pltpu.make_async_remote_copy(
            src_ref=view,
            dst_ref=view,
            send_sem=self.send.at[level, kind],
            recv_sem=self.recv.at[level, kind],
            device_id={"tp": w.across if kind == 1 else w.sibling},
        )

    def arrival(self, level, kind):
        w = self.where
        member = (w.sibling, w.across, w.corner)[kind]
        view = self.view(level, member)
        return pltpu.make_async_remote_copy(
            src_ref=view,
            dst_ref=view,
            send_sem=self.send.at[level, kind],
            recv_sem=self.recv.at[level, kind],
            device_id={"tp": w.across if kind == 1 else w.sibling},
        )

    def start(self, level):
        self.copy(level, 1).start()
        self.copy(level, 0).start()

    def relay(self, level):
        self.arrival(level, 1).wait_recv()
        self.copy(level, 2).start()

    def finish(self, level):
        self.arrival(level, 0).wait_recv()
        self.arrival(level, 2).wait_recv()

    def drain(self, level):
        for kind in range(3):
            self.copy(level, kind).wait_send()

    def pair_copy(self, incoming=False):
        w = self.where
        mine = self.view(0, w.member)
        other = self.view(1, w.member)
        return pltpu.make_async_remote_copy(
            src_ref=other if incoming else mine,
            dst_ref=other,
            send_sem=self.send.at[1, 3],
            recv_sem=self.recv.at[1, 3],
            device_id={"fs": w.pair},
        )


class RowScatter:
    def __init__(self, where, levels, rows, width, part, sends, recvs, semaphores, result):
        self.where = where
        self.levels = levels
        self.rows = rows
        self.width = width
        self.part = part
        self.sends = sends
        self.recvs = recvs
        self.send_sem, self.recv_sem = semaphores
        self.result = result

    def copy(self, block, stage):
        w = self.where
        device = ({"tp": w.sibling}, {"tp": w.across}, {"fs": w.pair})[stage]
        return pltpu.make_async_remote_copy(
            src_ref=self.sends[stage].at[block],
            dst_ref=self.recvs[stage].at[block],
            send_sem=self.send_sem.at[stage, block],
            recv_sem=self.recv_sem.at[stage, block],
            device_id=device,
        )

    def begin(self, block, value):
        w = self.where
        shape = (self.levels, 2, 2, self.rows, self.width)
        self.part[block] = value.reshape(shape)
        self.sends[0][block] = self.part[block, :, :, 1 - w.core].astype(BF16)
        self.copy(block, 0).start()

    def second(self, block):
        w = self.where
        self.copy(block, 0).wait_recv()
        away = self.part[block, :, 1 - w.chip, w.core]
        away = away + self.recvs[0][block, :, 1 - w.chip].astype(F32)
        self.sends[1][block] = away.astype(BF16)
        self.copy(block, 1).start()
        kept = self.part[block, :, w.chip, w.core]
        kept = kept + self.recvs[0][block, :, w.chip].astype(F32)
        self.part[block, :, 0, 0] = kept

    def third(self, block):
        self.copy(block, 1).wait_recv()
        if self.levels > 1:
            away = self.part[block, 1, 0, 0] + self.recvs[1][block, 1].astype(F32)
            self.sends[2][block] = away.astype(BF16)
            self.copy(block, 2).start()
            kept = self.part[block, 0, 0, 0] + self.recvs[1][block, 0].astype(F32)
            self.part[block, 0, 0, 0] = kept
        else:
            self.store(block, self.part[block, 0, 0, 0] + self.recvs[1][block, 0].astype(F32))

    def fourth(self, block):
        self.copy(block, 2).wait_recv()
        self.store(block, self.part[block, 0, 0, 0] + self.recvs[2][block].astype(F32))

    def store(self, block, value):
        self.result[:, rows_at(block * self.width, self.width, LANES)] = value

    def drain(self, block):
        for stage in range(1 + self.levels):
            self.copy(block, stage).wait_send()


def layer_kernel(sizes, *refs):
    (
        tokens,
        mix_gain,
        val_weight,
        gate_weight,
        conv_taps,
        chan_gain,
        out_weight,
        mix_post_gain,
        ffn_gain,
        up_gate_weight,
        up_val_weight,
        ffn_taps,
        down_weight,
        ffn_post_gain,
        layer_out,
        tokens_in,
        conv_taps_in,
        ffn_taps_in,
        mix_gain_in,
        chan_gain_in,
        mix_post_gain_in,
        ffn_gain_in,
        ffn_post_gain_in,
        val_all,
        gate_all,
        out_all,
        up_gate_all,
        up_val_all,
        down_all,
        mix_rows,
        ffn_rows,
        glu_padded,
        conv_out,
        stats,
        activated,
        up_padded,
        hidden,
        residual_ref,
        result,
        mix_part,
        ffn_part,
        mix_send0,
        mix_send1,
        mix_recv0,
        mix_recv1,
        ffn_send0,
        ffn_send1,
        ffn_send2,
        ffn_recv0,
        ffn_recv1,
        ffn_recv2,
        out_staged,
        load_sem,
        own_sem,
        z_send,
        z_recv,
        y_send,
        y_recv,
        mix_row_send,
        mix_row_recv,
        ffn_row_send,
        ffn_row_recv,
        stat_send,
        stat_recv,
        mix_sum_send,
        mix_sum_recv,
        ffn_sum_send,
        ffn_sum_recv,
    ) = refs
    w = Where()
    rows, group_rows, segments = sizes["rows"], sizes["group_rows"], sizes["segments"]
    depth, local_ch, half_ff = sizes["depth"], sizes["local_ch"], sizes["half_ff"]
    width = out_all.shape[2]
    mix_tiles, ffn_tiles = local_ch // LANES, half_ff // LANES
    member = w.member

    barrier = pltpu.get_barrier_semaphore()
    friends = [
        {"tp": w.sibling},
        {"tp": w.across},
        {"tp": w.corner},
        {"grp": 1 - w.half},
        {"fs": w.mate},
        {"fs": w.pair},
    ]
    for friend in friends:
        pl.semaphore_signal(barrier, inc=1, device_id=friend)

    @pl.when(w.inner)
    def _():
        pl.semaphore_signal(barrier, inc=1, device_id={"fs": 3 - w.place})

    pieces = []

    def cut(source, held, sided, chunks):
        total = held.shape[1] // 2
        size = total // chunks
        return [
            Piece(source, held, index * size, size, total, sided, held.shape[2])
            for index in range(chunks)
        ]

    val_pieces = cut(val_weight, val_all, None, 2)
    gate_pieces = cut(gate_weight, gate_all, None, 2)
    out_pieces = cut(out_weight, out_all, None, 2)
    up_gate_pieces = cut(up_gate_weight, up_gate_all, "columns", 2)
    up_val_pieces = cut(up_val_weight, up_val_all, "columns", 2)
    down_pieces = cut(down_weight, down_all, "rows", sizes["down_chunks"])
    first = [val_pieces[0], gate_pieces[0], val_pieces[1], gate_pieces[1]]
    later = [up_gate_pieces[0], up_val_pieces[0], up_gate_pieces[1], up_val_pieces[1]]
    pieces = first + out_pieces + later + down_pieces
    proj = list(range(0, 4))
    outs = list(range(4, 6))
    ups = list(range(6, 10))
    downs = list(range(10, 10 + len(down_pieces)))
    stream = Stream(w, pieces, (z_send, z_recv, y_send, y_recv))

    def own_copy(index, source, held, sided):
        if sided == "columns":
            view = source.at[:, rows_at(w.side * held.shape[2], held.shape[2], LANES)]
        elif sided == "rows":
            view = source.at[rows_at(w.side * held.shape[1], held.shape[1])]
        else:
            view = source
        return pltpu.make_async_copy(view, held.at[w.place], own_sem.at[index])

    own_copies = [
        own_copy(0, val_weight, val_all, None),
        own_copy(1, gate_weight, gate_all, None),
        own_copy(2, out_weight, out_all, None),
        own_copy(3, up_gate_weight, up_gate_all, "columns"),
        own_copy(4, up_val_weight, up_val_all, "columns"),
        own_copy(5, down_weight, down_all, "rows"),
    ]
    small = [
        (tokens, tokens_in),
        (mix_gain, mix_gain_in),
        (conv_taps, conv_taps_in),
        (chan_gain, chan_gain_in),
        (mix_post_gain, mix_post_gain_in),
        (ffn_gain, ffn_gain_in),
        (ffn_taps, ffn_taps_in),
        (ffn_post_gain, ffn_post_gain_in),
    ]
    loads = [
        pltpu.make_async_copy(source, held, load_sem.at[index])
        for index, (source, held) in enumerate(small)
    ]
    for copy in loads + own_copies:
        copy.start()

    glu_padded[:, 0:32, :] = jnp.zeros((glu_padded.shape[0], 32, LANES), F32)
    up_padded[:, :, 0:8, :] = jnp.zeros((2, up_padded.shape[1], 8, LANES), F32)
    own_rows = rows_at(member * rows, rows)

    def gain_of(held):
        return held[...].astype(F32).reshape(1, held.shape[0])

    loads[0].wait()
    loads[1].wait()
    mix_rows[own_rows] = rms_scale(tokens_in[...].astype(F32), gain_of(mix_gain_in)).astype(BF16)

    pl.semaphore_wait(barrier, len(friends) + w.inner.astype(jnp.int32))

    ahead = 2
    for unit in range(ahead):
        stream.start(unit)
    mix_gather = RowGather(w, mix_rows, rows, group_rows, (mix_row_send, mix_row_recv))
    mix_gather.start(0)
    stream.events(list(range(len(pieces))), ahead, 2)
    stream.pump(9)
    mix_gather.relay(0)
    stream.pump(8)
    for unit in proj:
        stream.arrive(unit)
    own_copies[0].wait()
    own_copies[1].wait()
    mix_gather.finish(0)

    left = mix_rows[...]
    values = product(left, val_all[...].reshape(depth, local_ch))
    gate_sums = product(left, gate_all[...].reshape(depth, local_ch))
    glu = (values * jax.nn.sigmoid(gate_sums)).astype(BF16).astype(F32)
    for tile in range(mix_tiles):
        block = glu[:, tile * LANES : (tile + 1) * LANES].reshape(segments, LEN, LANES)
        glu_padded[tile * segments : (tile + 1) * segments, 32:, :] = block
    stream.pump(1)

    taps_count = conv_taps.shape[0]
    loads[2].wait()
    loads[3].wait()
    for tile in range(mix_tiles):
        lanes = rows_at(member * local_ch + tile * LANES, LANES, LANES)
        taps = conv_taps_in[:, lanes].astype(F32)

        @pl.loop(0, segments)
        def _(segment):
            total = jnp.zeros((LEN, LANES), F32)
            for k in range(taps_count):
                shifted = glu_padded[tile * segments + segment, pl.ds(33 - taps_count + k, LEN), :]
                total = total + shifted * taps[k : k + 1]
            conv_out[tile, rows_at(segment * LEN, LEN)] = total

    sums = conv_out[0]
    squares = conv_out[0] * conv_out[0]
    for tile in range(1, mix_tiles):
        sums = sums + conv_out[tile]
        squares = squares + conv_out[tile] * conv_out[tile]
    exact = lax.Precision.HIGHEST
    ones = jnp.ones((8, LANES), F32)
    contract_lanes = (((1,), (1,)), ((), ()))
    sums = lax.dot_general(ones, sums, contract_lanes, precision=exact, preferred_element_type=F32)
    squares = lax.dot_general(
        ones, squares, contract_lanes, precision=exact, preferred_element_type=F32
    )
    upper = lax.broadcasted_iota(jnp.int32, (8, group_rows), 0) < 4
    stats[0, :, :] = jnp.zeros(stats.shape[1:], F32)
    stats[0, :, 0:group_rows] = jnp.where(upper, sums, squares)

    def stat_copy(kind):
        device = (w.sibling, w.across, w.corner)[kind]
        return pltpu.make_async_remote_copy(
            src_ref=stats.at[0],
            dst_ref=stats.at[1 + kind],
            send_sem=stat_send.at[kind],
            recv_sem=stat_recv.at[kind],
            device_id={"tp": device},
        )

    for kind in (2, 1, 0):
        stat_copy(kind).start()
    stream.pump(2)
    for unit in outs:
        stream.arrive(unit)
    own_copies[2].wait()
    for kind in range(3):
        stat_copy(kind).wait_recv()
    total = stats[0] + stats[1] + stats[2] + stats[3]
    flipped = jnp.transpose(total)[:group_rows] / chan_gain.shape[0]
    chan_mean = flipped[:, 0:1]
    chan_var = flipped[:, 4:5] - chan_mean * chan_mean
    inverse = lax.rsqrt(chan_var + chan_epsilon)
    chan_gains = chan_gain_in[rows_at(member * local_ch, local_ch, LANES)].astype(F32)
    chan_gains = chan_gains.reshape(1, local_ch)
    for tile in range(mix_tiles):
        scaled = (conv_out[tile] - chan_mean) * inverse * chan_gains[:, tile * LANES : (tile + 1) * LANES]
        activated[:, tile * LANES : (tile + 1) * LANES] = jax.nn.silu(scaled).astype(BF16)

    mix_sum = RowScatter(
        w,
        1,
        rows,
        width,
        mix_part,
        (mix_send0, mix_send1),
        (mix_recv0, mix_recv1),
        (mix_sum_send, mix_sum_recv),
        result,
    )
    places = [w.place, w.mate, w.source(3), w.source(2)]
    for index in range(4 + 2):
        if index < 4:
            block = places[index]
            mix_sum.begin(block, product(activated[...], out_all[block]))
        if 1 <= index < 5:
            mix_sum.second(places[index - 1])
        if 2 <= index:
            mix_sum.third(places[index - 2])
        if index % 2 == 1:
            stream.pump(1)

    loads[4].wait()
    loads[5].wait()
    residual = tokens_in[...].astype(F32) + rms_scale(result[...], gain_of(mix_post_gain_in))
    residual = residual.astype(BF16)
    residual_ref[...] = residual
    ffn_rows[own_rows] = rms_scale(residual.astype(F32), gain_of(ffn_gain_in)).astype(BF16)
    ffn_gather = RowGather(w, ffn_rows, rows, group_rows, (ffn_row_send, ffn_row_recv))
    ffn_gather.start(0)
    ffn_gather.pair_copy().start()
    stream.pump(1)
    ffn_gather.relay(0)
    stream.pump(2)
    ffn_gather.pair_copy(incoming=True).wait_recv()
    ffn_gather.start(1)
    stream.pump(2)
    ffn_gather.relay(1)
    stream.pump(6)
    for unit in ups:
        stream.arrive(unit)
    own_copies[3].wait()
    own_copies[4].wait()
    loads[6].wait()

    def feed(level):
        ffn_gather.finish(level)
        left = ffn_rows[level * group_rows : (level + 1) * group_rows]
        for half, weight in enumerate((up_gate_all, up_val_all)):
            up = product(left, weight[...].reshape(depth, half_ff)).astype(BF16).astype(F32)
            for tile in range(ffn_tiles):
                block = up[:, tile * LANES : (tile + 1) * LANES].reshape(segments, LEN, LANES)
                up_padded[half, tile * segments : (tile + 1) * segments, 8:, :] = block
            stream.pump(1)
        for tile in range(ffn_tiles):
            first_lane = (2 * member + w.side) * half_ff + tile * LANES
            lanes = rows_at(first_lane, LANES, LANES)
            taps = [ffn_taps_in[:, half, lanes].astype(F32) for half in range(2)]

            @pl.loop(0, segments)
            def _(segment):
                convs = []
                for half in range(2):
                    conv = jnp.zeros((LEN, LANES), F32)
                    count = ffn_taps.shape[0]
                    for k in range(count):
                        shifted = up_padded[
                            half, tile * segments + segment, pl.ds(9 - count + k, LEN), :
                        ]
                        conv = conv + shifted * taps[half][k : k + 1]
                    convs.append(conv)
                value = jax.nn.gelu(convs[0], approximate=True) * convs[1]
                at = rows_at(level * group_rows + segment * LEN, LEN)
                hidden[at, tile * LANES : (tile + 1) * LANES] = value.astype(BF16)

    feed(0)
    stream.pump(1)
    feed(1)
    ffn_sum = RowScatter(
        w,
        2,
        rows,
        width,
        ffn_part,
        (ffn_send0, ffn_send1, ffn_send2),
        (ffn_recv0, ffn_recv1, ffn_recv2),
        (ffn_sum_send, ffn_sum_recv),
        result,
    )
    own_copies[5].wait()
    slots = [None, 1, 3, 2]
    stream.pump(1)
    for index in range(4 + 2):
        if index < 4:
            block = places[index]
            if index == 1:
                stream.pump(len(stream.waiting))
            if index > 0:
                for unit in downs:
                    stream.y_copy(unit, slots[index], incoming=True).wait_recv()
            ffn_sum.begin(block, product(hidden[...], down_all[block]))
        if 1 <= index < 5:
            ffn_sum.second(places[index - 1])
        if 2 <= index:
            ffn_sum.third(places[index - 2])
    for index in (3, 2, 1, 0):
        ffn_sum.fourth(places[3 - index])
    loads[7].wait()
    final = residual_ref[...].astype(F32) + rms_scale(result[...], gain_of(ffn_post_gain_in))
    out_staged[...] = final.astype(BF16)
    leave = pltpu.make_async_copy(out_staged, layer_out, load_sem.at[len(small)])
    leave.start()

    for unit in range(len(pieces)):
        stream.drain(unit)
    mix_gather.drain(0)
    ffn_gather.drain(0)
    ffn_gather.drain(1)
    ffn_gather.pair_copy().wait_send()
    for kind in range(3):
        stat_copy(kind).wait_send()
    for index in range(4):
        mix_sum.drain(places[index])
        ffn_sum.drain(places[index])
    leave.wait()


def kernel_sizes(tokens, val_weight, out_weight, up_gate_weight, down_weight):
    rows = tokens.shape[0]
    return {
        "rows": rows,
        "group_rows": 4 * rows,
        "segments": 4 * rows // LEN,
        "depth": 4 * val_weight.shape[0],
        "local_ch": val_weight.shape[1],
        "half_ff": up_gate_weight.shape[1] // 2,
        "down_chunks": 4,
    }


def run_kernel(*args):
    (
        tokens,
        mix_gain,
        val_weight,
        gate_weight,
        conv_taps,
        chan_gain,
        out_weight,
        mix_post_gain,
        ffn_gain,
        up_gate_weight,
        up_val_weight,
        ffn_taps,
        down_weight,
        ffn_post_gain,
    ) = args
    sizes = kernel_sizes(tokens, val_weight, out_weight, up_gate_weight, down_weight)
    rows, group_rows, segments = sizes["rows"], sizes["group_rows"], sizes["segments"]
    local_ch, half_ff = sizes["local_ch"], sizes["half_ff"]
    width = out_weight.shape[1]
    model = tokens.shape[1]
    mix_tiles, ffn_tiles = local_ch // LANES, half_ff // LANES
    padded_rows = -(-group_rows // LANES) * LANES
    units = 10 + sizes["down_chunks"]
    dma = pltpu.SemaphoreType.DMA
    shaped = [
        tokens,
        mix_gain,
        val_weight,
        gate_weight,
        conv_taps,
        chan_gain,
        out_weight,
        mix_post_gain,
        ffn_gain,
        up_gate_weight,
        up_val_weight,
        jnp.transpose(ffn_taps, (1, 0, 2)),
        down_weight,
        ffn_post_gain,
    ]
    scratch = [
        pltpu.VMEM(tokens.shape, BF16),
        pltpu.VMEM(conv_taps.shape, BF16),
        pltpu.VMEM(shaped[11].shape, BF16),
        pltpu.VMEM(mix_gain.shape, BF16),
        pltpu.VMEM(chan_gain.shape, BF16),
        pltpu.VMEM(mix_post_gain.shape, BF16),
        pltpu.VMEM(ffn_gain.shape, BF16),
        pltpu.VMEM(ffn_post_gain.shape, BF16),
        pltpu.VMEM((4, val_weight.shape[0], local_ch), BF16),
        pltpu.VMEM((4, gate_weight.shape[0], local_ch), BF16),
        pltpu.VMEM((4, local_ch, width), BF16),
        pltpu.VMEM((4, up_gate_weight.shape[0], half_ff), BF16),
        pltpu.VMEM((4, up_val_weight.shape[0], half_ff), BF16),
        pltpu.VMEM((4, half_ff, width), BF16),
        pltpu.VMEM((group_rows, model), BF16),
        pltpu.VMEM((2 * group_rows, model), BF16),
        pltpu.VMEM((mix_tiles * segments, 32 + LEN, LANES), F32),
        pltpu.VMEM((mix_tiles, group_rows, LANES), F32),
        pltpu.VMEM((4, 8, padded_rows), F32),
        pltpu.VMEM((group_rows, local_ch), BF16),
        pltpu.VMEM((2, ffn_tiles * segments, 8 + LEN, LANES), F32),
        pltpu.VMEM((2 * group_rows, half_ff), BF16),
        pltpu.VMEM((rows, model), BF16),
        pltpu.VMEM((rows, model), F32),
        pltpu.VMEM((4, 1, 2, 2, rows, width), F32),
        pltpu.VMEM((4, 2, 2, 2, rows, width), F32),
        pltpu.VMEM((4, 1, 2, rows, width), BF16),
        pltpu.VMEM((4, 1, rows, width), BF16),
        pltpu.VMEM((4, 1, 2, rows, width), BF16),
        pltpu.VMEM((4, 1, rows, width), BF16),
        pltpu.VMEM((4, 2, 2, rows, width), BF16),
        pltpu.VMEM((4, 2, rows, width), BF16),
        pltpu.VMEM((4, rows, width), BF16),
        pltpu.VMEM((4, 2, 2, rows, width), BF16),
        pltpu.VMEM((4, 2, rows, width), BF16),
        pltpu.VMEM((4, rows, width), BF16),
        pltpu.VMEM(tokens.shape, BF16),
        dma((9,)),
        dma((6,)),
        dma((units, 4)),
        dma((units, 3)),
        dma((units, 3)),
        dma((units, 3)),
        dma((1, 3)),
        dma((1, 3)),
        dma((2, 4)),
        dma((2, 4)),
        dma((3,)),
        dma((3,)),
        dma((2, 4)),
        dma((2, 4)),
        dma((3, 4)),
        dma((3, 4)),
    ]
    return pl.pallas_call(
        functools.partial(layer_kernel, sizes),
        out_shape=jax.ShapeDtypeStruct(tokens.shape, BF16),
        in_specs=[pl.BlockSpec(memory_space=pltpu.HBM)] * len(shaped),
        out_specs=pl.BlockSpec(memory_space=pl.ANY),
        scratch_shapes=scratch,
        compiler_params=pltpu.CompilerParams(
            collective_id=0, has_side_effects=True, vmem_limit_bytes=67_043_328
        ),
    )(*shaped)


def fits(mesh, args):
    tokens, val_weight, out_weight = args[0], args[2], args[6]
    up_gate_weight, down_weight = args[9], args[12]
    if (mesh.shape["grp"], mesh.shape["fs"], mesh.shape["tp"]) != (2, 4, 4):
        return False
    rows = tokens.shape[0] // 32
    local_ch, local_ff = val_weight.shape[1] // 4, up_gate_weight.shape[1] // 4
    local_model = tokens.shape[1] // 4
    return (
        rows % 16 == 0
        and 4 * rows % LEN == 0
        and local_ch % LANES == 0
        and local_ff % (2 * LANES) == 0
        and local_model % LANES == 0
        and args[4].shape[0] <= 32
        and args[11].shape[1] <= 8
    )


def solution(mesh):
    specs = (
        P(("grp", "fs", "tp"), None),
        P(),
        P("fs", "tp"),
        P("fs", "tp"),
        P(),
        P(),
        P("tp", "fs"),
        P(),
        P(),
        P("fs", "tp"),
        P("fs", "tp"),
        P(),
        P("tp", "fs"),
        P(),
    )

    def whole(*args):
        body = run_kernel if fits(mesh, args) else plain
        step = jax.shard_map(
            body,
            mesh=mesh,
            in_specs=specs,
            out_specs=P(("grp", "fs", "tp"), None),
            check_vma=False,
        )
        return step(*args)

    return whole
```

```python
import functools

import jax
import jax.numpy as jnp
from jax import lax
from jax.experimental import pallas as pl
from jax.experimental.pallas import tpu as pltpu
from jax.sharding import PartitionSpec as P

LEN = 64
LANES = 128
SUMS = 1
UP_CUTS = 4
AHEAD = 2
F32 = jnp.float32
BF16 = jnp.bfloat16

norm_epsilon = 1e-06
chan_epsilon = 1e-05


def rms_scale(values, gain):
    inverse = lax.rsqrt(jnp.mean(values * values, axis=-1, keepdims=True) + norm_epsilon)
    return values * inverse * gain.astype(F32)


def depthwise(signal, tap_table):
    taps_count = tap_table.shape[0]
    channels = signal.shape[1]
    shaped = signal.astype(F32).reshape(signal.shape[0] // LEN, LEN, channels)
    padded = jnp.pad(shaped, ((0, 0), (taps_count - 1, 0), (0, 0)))
    tap_values = tap_table.astype(F32)
    result = jnp.zeros(shaped.shape, F32)
    for offset in range(taps_count):
        result = result + padded[:, offset : offset + LEN, :] * tap_values[offset]
    return result.reshape(signal.shape[0], channels)


def gather_rows(weight):
    return lax.all_gather(weight, "fs", axis=0, tiled=True)


def gather_columns(weight):
    return lax.all_gather(weight, "fs", axis=1, tiled=True)


def product(left, right):
    return jnp.dot(left, right, preferred_element_type=F32)


def scatter_sum(part):
    return lax.psum_scatter(
        part.astype(BF16), "tp", scatter_dimension=0, tiled=True
    ).astype(F32)


def plain(
    tokens,
    mix_gain,
    val_weight,
    gate_weight,
    conv_taps,
    chan_gain,
    out_weight,
    mix_post_gain,
    ffn_gain,
    up_gate_weight,
    up_val_weight,
    ffn_taps,
    down_weight,
    ffn_post_gain,
):
    member = lax.axis_index("tp")
    normed_own = rms_scale(tokens.astype(F32), mix_gain).astype(BF16)
    normed = lax.all_gather(normed_own, "tp", axis=0, tiled=True)
    local_ch = val_weight.shape[1]
    values = product(normed, gather_rows(val_weight))
    gate_sums = product(normed, gather_rows(gate_weight))
    glu_out = (values * jax.nn.sigmoid(gate_sums)).astype(BF16)
    own_taps = lax.dynamic_slice_in_dim(conv_taps, member * local_ch, local_ch, 1)
    conv_out = depthwise(glu_out, own_taps)
    totals, squares = lax.psum(
        (jnp.sum(conv_out, axis=1), jnp.sum(conv_out * conv_out, axis=1)), "tp"
    )
    all_channels = chan_gain.shape[0]
    chan_mean = totals[:, None] / all_channels
    chan_var = squares[:, None] / all_channels - chan_mean * chan_mean
    own_gain = lax.dynamic_slice_in_dim(chan_gain, member * local_ch, local_ch, 0).astype(F32)
    activated = jax.nn.silu((conv_out - chan_mean) * lax.rsqrt(chan_var + chan_epsilon) * own_gain)
    mixed_sum = scatter_sum(product(activated.astype(BF16), gather_columns(out_weight)))
    residual = (tokens.astype(F32) + rms_scale(mixed_sum, mix_post_gain)).astype(BF16)
    normed_share = rms_scale(residual.astype(F32), ffn_gain).astype(BF16)
    normed_ffn = lax.all_gather(normed_share, "tp", axis=0, tiled=True)
    local_ff = up_gate_weight.shape[1]
    own_ffn_taps = lax.dynamic_slice_in_dim(ffn_taps, member * local_ff, local_ff, 2)
    up_gate = product(normed_ffn, gather_rows(up_gate_weight)).astype(BF16)
    up_val = product(normed_ffn, gather_rows(up_val_weight)).astype(BF16)
    gate_conv = depthwise(up_gate, own_ffn_taps[0])
    val_conv = depthwise(up_val, own_ffn_taps[1])
    hidden = (jax.nn.gelu(gate_conv, approximate=True) * val_conv).astype(BF16)
    ffn_sum = scatter_sum(product(hidden, gather_columns(down_weight)))
    return (residual.astype(F32) + rms_scale(ffn_sum, ffn_post_gain)).astype(BF16)


def rows_at(start, size, unit=16):
    return pl.ds(pl.multiple_of(start, unit), size)


class Where:
    def __init__(self):
        self.place = lax.axis_index("fs")
        self.half = lax.axis_index("grp")
        self.member = lax.axis_index("tp")
        place, member = self.place, self.member
        self.side = place // 2
        self.inner = jnp.logical_or(place == 1, place == 2)
        self.chip = member // 2
        self.core = member % 2
        self.mate = place + 1 - 2 * (place % 2)
        self.over = 2 - self.side
        self.pair = lax.rem(place + 2, 4)
        self.sibling = member + 1 - 2 * self.core
        self.across = lax.rem(member + 2, 4)
        self.corner = self.sibling + 2 - 4 * self.chip

    def source(self, slot):
        if slot == 1:
            return self.mate
        if slot == 2:
            return self.pair
        return self.pair + 1 - 2 * (self.place % 2)


class Piece:
    def __init__(self, source, held, start, size, stride, sided, columns, lanes=None):
        self.source_ref = source
        self.held = held
        self.start = start
        self.size = size
        self.stride = stride
        self.sided = sided
        self.columns = columns
        self.lanes = lanes

    def read(self, where, side):
        first = where.half * self.stride + self.start
        if self.sided == "rows":
            first = side * (2 * self.stride) + first
        rows = rows_at(first, self.size)
        if self.sided == "columns":
            columns = rows_at(side * self.columns, self.columns, LANES)
            return self.source_ref.at[rows, columns]
        if self.lanes is not None:
            return self.source_ref.at[rows, self.lanes]
        return self.source_ref.at[rows]

    def target(self, where, origin, half):
        first = half * self.stride + self.start
        rows = rows_at(first, self.size)
        if self.lanes is not None:
            return self.held.at[origin, rows, self.lanes]
        return self.held.at[origin, rows]


class Stream:
    def __init__(self, where, pieces, semaphores):
        self.where = where
        self.pieces = pieces
        self.z_send, self.z_recv, self.y_send, self.y_recv = semaphores

    def z_copy(self, unit, kind):
        w, piece = self.where, self.pieces[unit]
        if kind < 2:
            side = w.side if kind == 0 else 1 - w.side
            source = piece.read(w, side)
            target = piece.target(w, w.place, w.half)
            device = w.mate if kind == 0 else w.over
            if kind == 0:
                slot = 1
            else:
                slot = 2 + w.inner.astype(jnp.int32)
        else:
            target = piece.target(w, w.source(kind), w.half)
            source = target
            device = w.mate
            slot = 5 - kind
        return pltpu.make_async_remote_copy(
            src_ref=source,
            dst_ref=target,
            send_sem=self.z_send.at[unit, kind],
            recv_sem=self.z_recv.at[unit, slot - 1],
            device_id={"fs": device},
        )

    def z_arrival(self, unit, slot):
        w = self.where
        target = self.pieces[unit].target(w, w.source(slot), w.half)
        return pltpu.make_async_remote_copy(
            src_ref=target,
            dst_ref=target,
            send_sem=self.z_send.at[unit, 0],
            recv_sem=self.z_recv.at[unit, slot - 1],
            device_id={"fs": w.mate},
        )

    def y_copy(self, unit, slot, incoming=False):
        w = self.where
        half = 1 - w.half if incoming else w.half
        target = self.pieces[unit].target(w, w.source(slot), half)
        return pltpu.make_async_remote_copy(
            src_ref=target,
            dst_ref=target,
            send_sem=self.y_send.at[unit, slot - 1],
            recv_sem=self.y_recv.at[unit, slot - 1],
            device_id={"grp": 1 - w.half},
        )

    def start(self, unit):
        self.z_copy(unit, 0).start()
        self.z_copy(unit, 1).start()

    def serve(self, unit, slot, relay):
        self.z_arrival(unit, slot).wait_recv()
        if relay:
            self.z_copy(unit, slot).start()
        self.y_copy(unit, slot).start()

    def events(self, order, tail, ahead, lag):
        count, body = len(order), len(order) - tail
        inner, outer = [], []
        for index in range(count + lag):
            first = [order[index + ahead]] if index + ahead < count else []
            if index == body - 1:
                first = order[index + ahead :]
            elif index >= body:
                first = []
            if index < body:
                inner.append((first, order[index], 2, True))
                inner.append(([], order[index], 3, True))
                inner.append(([], order[index], 1, False))
            if index < count:
                outer.append((first, order[index], 1, False))
            if lag <= index < body + lag:
                outer.append(([], order[index - lag], 3, False))
                outer.append(([], order[index - lag], 2, False))
        last = order[body:]
        for slot in (3, 1, 2):
            inner += [([], unit, slot, slot > 1) for unit in last]
        for slot in (2, 3):
            outer += [([], unit, slot, False) for unit in last]
        self.waiting = list(zip(inner, outer))

    def pump_until(self, left):
        self.pump(max(0, len(self.waiting) - left))

    def pump(self, count):
        for _ in range(min(count, len(self.waiting))):
            pair = self.waiting.pop(0)
            for role, (begin, unit, slot, relay) in enumerate(pair):
                chosen = jnp.logical_not(self.where.inner) if role else self.where.inner

                @pl.when(chosen)
                def _():
                    for other in begin:
                        self.start(other)
                    self.serve(unit, slot, relay)

    def arrive(self, unit):
        for slot in (1, 3, 2):
            self.y_copy(unit, slot, incoming=True).wait_recv()

    def drain(self, unit):
        self.z_copy(unit, 0).wait_send()
        self.z_copy(unit, 1).wait_send()
        for slot in (1, 2, 3):
            if slot > 1:

                @pl.when(self.where.inner)
                def _():
                    self.z_copy(unit, slot).wait_send()

            self.y_copy(unit, slot).wait_send()


class RowGather:
    def __init__(self, where, held, rows, group_rows, semaphores):
        self.where = where
        self.held = held
        self.rows = rows
        self.group_rows = group_rows
        self.send, self.recv = semaphores

    def view(self, level, member):
        first = level * self.group_rows + member * self.rows
        return self.held.at[rows_at(first, self.rows)]

    def copy(self, level, kind):
        w = self.where
        view = self.view(level, w.across if kind == 2 else w.member)
        return pltpu.make_async_remote_copy(
            src_ref=view,
            dst_ref=view,
            send_sem=self.send.at[level, kind],
            recv_sem=self.recv.at[level, kind],
            device_id={"tp": w.across if kind == 1 else w.sibling},
        )

    def arrival(self, level, kind):
        w = self.where
        member = (w.sibling, w.across, w.corner)[kind]
        view = self.view(level, member)
        return pltpu.make_async_remote_copy(
            src_ref=view,
            dst_ref=view,
            send_sem=self.send.at[level, kind],
            recv_sem=self.recv.at[level, kind],
            device_id={"tp": w.across if kind == 1 else w.sibling},
        )

    def start(self, level):
        self.copy(level, 1).start()
        self.copy(level, 0).start()

    def relay(self, level):
        self.arrival(level, 1).wait_recv()
        self.copy(level, 2).start()

    def finish(self, level):
        self.arrival(level, 0).wait_recv()
        self.arrival(level, 2).wait_recv()

    def drain(self, level):
        for kind in range(3):
            self.copy(level, kind).wait_send()

    def pair_copy(self, incoming=False):
        w = self.where
        mine = self.view(0, w.member)
        other = self.view(1, w.member)
        return pltpu.make_async_remote_copy(
            src_ref=other if incoming else mine,
            dst_ref=other,
            send_sem=self.send.at[1, 3],
            recv_sem=self.recv.at[1, 3],
            device_id={"fs": w.pair},
        )


class RowScatter:
    def __init__(self, where, levels, rows, width, part, sends, recvs, semaphores, result):
        self.where = where
        self.levels = levels
        self.rows = rows
        self.width = width
        self.part = part
        self.sends = sends
        self.recvs = recvs
        self.send_sem, self.recv_sem = semaphores
        self.result = result

    def copy(self, block, stage):
        w = self.where
        device = ({"tp": w.sibling}, {"tp": w.across}, {"fs": w.pair})[stage]
        return pltpu.make_async_remote_copy(
            src_ref=self.sends[stage].at[block],
            dst_ref=self.recvs[stage].at[block],
            send_sem=self.send_sem.at[stage, block],
            recv_sem=self.recv_sem.at[stage, block],
            device_id=device,
        )

    def begin(self, block, value):
        w = self.where
        shape = (self.levels, 2, 2, self.rows, self.width)
        self.part[block] = value.reshape(shape)
        self.sends[0][block] = self.part[block, :, :, 1 - w.core].astype(BF16)
        self.copy(block, 0).start()

    def second(self, block):
        w = self.where
        self.copy(block, 0).wait_recv()
        away = self.part[block, :, 1 - w.chip, w.core]
        away = away + self.recvs[0][block, :, 1 - w.chip].astype(F32)
        self.sends[1][block] = away.astype(BF16)
        self.copy(block, 1).start()
        kept = self.part[block, :, w.chip, w.core]
        kept = kept + self.recvs[0][block, :, w.chip].astype(F32)
        self.part[block, :, 0, 0] = kept

    def third(self, block):
        self.copy(block, 1).wait_recv()
        if self.levels > 1:
            away = self.part[block, 1, 0, 0] + self.recvs[1][block, 1].astype(F32)
            self.sends[2][block] = away.astype(BF16)
            self.copy(block, 2).start()
            kept = self.part[block, 0, 0, 0] + self.recvs[1][block, 0].astype(F32)
            self.part[block, 0, 0, 0] = kept
        else:
            self.store(block, self.part[block, 0, 0, 0] + self.recvs[1][block, 0].astype(F32))

    def fourth(self, block):
        self.copy(block, 2).wait_recv()
        self.store(block, self.part[block, 0, 0, 0] + self.recvs[2][block].astype(F32))

    def store(self, block, value):
        self.result[:, rows_at(block * self.width, self.width, LANES)] = value

    def drain(self, block):
        for stage in range(1 + self.levels):
            self.copy(block, stage).wait_send()


def layer_kernel(sizes, *refs):
    (
        tokens,
        mix_gain,
        val_weight,
        gate_weight,
        conv_taps,
        chan_gain,
        out_weight,
        mix_post_gain,
        ffn_gain,
        up_gate_weight,
        up_val_weight,
        ffn_taps,
        down_weight,
        ffn_post_gain,
        layer_out,
        tokens_in,
        conv_taps_in,
        ffn_taps_in,
        mix_gain_in,
        chan_gain_in,
        mix_post_gain_in,
        ffn_gain_in,
        ffn_post_gain_in,
        val_all,
        gate_all,
        out_all,
        up_gate_all,
        up_val_all,
        down_all,
        mix_rows,
        ffn_rows,
        glu_padded,
        conv_out,
        stats,
        activated,
        up_padded,
        hidden,
        residual_ref,
        result,
        mix_part,
        ffn_part,
        mix_send0,
        mix_send1,
        mix_recv0,
        mix_recv1,
        ffn_send0,
        ffn_send1,
        ffn_send2,
        ffn_recv0,
        ffn_recv1,
        ffn_recv2,
        out_staged,
        load_sem,
        own_sem,
        z_send,
        z_recv,
        y_send,
        y_recv,
        mix_row_send,
        mix_row_recv,
        ffn_row_send,
        ffn_row_recv,
        stat_send,
        stat_recv,
        mix_sum_send,
        mix_sum_recv,
        ffn_sum_send,
        ffn_sum_recv,
    ) = refs
    w = Where()
    rows, group_rows, segments = sizes["rows"], sizes["group_rows"], sizes["segments"]
    depth, local_ch, half_ff = sizes["depth"], sizes["local_ch"], sizes["half_ff"]
    width = out_all.shape[2] // SUMS
    mix_tiles, ffn_tiles = local_ch // LANES, half_ff // LANES
    member = w.member

    barrier = pltpu.get_barrier_semaphore()
    friends = [
        {"tp": w.sibling},
        {"tp": w.across},
        {"tp": w.corner},
        {"grp": 1 - w.half},
        {"fs": w.mate},
        {"fs": w.pair},
    ]
    for friend in friends:
        pl.semaphore_signal(barrier, inc=1, device_id=friend)

    @pl.when(w.inner)
    def _():
        pl.semaphore_signal(barrier, inc=1, device_id={"fs": 3 - w.place})

    pieces = []

    def cut(source, held, sided, chunks):
        total = held.shape[1] // 2
        size = total // chunks
        return [
            Piece(source, held, index * size, size, total, sided, held.shape[2])
            for index in range(chunks)
        ]

    val_pieces = cut(val_weight, val_all, None, 2)
    gate_pieces = cut(gate_weight, gate_all, None, 2)
    out_pieces = cut(out_weight, out_all, None, 2)
    up_gate_pieces = cut(up_gate_weight, up_gate_all, "columns", UP_CUTS)
    up_val_pieces = cut(up_val_weight, up_val_all, "columns", UP_CUTS)
    down_rows = half_ff // 2
    down_size = down_rows // 2
    down_pieces = [
        Piece(
            down_weight,
            down_all,
            row * down_size,
            down_size,
            down_rows,
            "rows",
            None,
            pl.ds(part * width, width),
        )
        for part in range(SUMS)
        for row in range(2)
    ]
    mixed = [piece for pair in zip(val_pieces, gate_pieces) for piece in pair]
    upward = [piece for pair in zip(up_gate_pieces, up_val_pieces) for piece in pair]
    pieces = mixed + out_pieces + upward + down_pieces
    proj = list(range(0, 4))
    outs = list(range(4, 6))
    ups = list(range(6, 6 + len(upward)))
    downs = list(range(6 + len(upward), len(pieces)))
    stream = Stream(w, pieces, (z_send, z_recv, y_send, y_recv))

    def own_copy(index, source, held, sided):
        if sided == "columns":
            view = source.at[:, rows_at(w.side * held.shape[2], held.shape[2], LANES)]
        elif sided == "rows":
            view = source.at[rows_at(w.side * held.shape[1], held.shape[1])]
        else:
            view = source
        return pltpu.make_async_copy(view, held.at[w.place], own_sem.at[index])

    own_copies = [
        own_copy(0, val_weight, val_all, None),
        own_copy(1, gate_weight, gate_all, None),
        own_copy(2, out_weight, out_all, None),
        own_copy(3, up_gate_weight, up_gate_all, "columns"),
        own_copy(4, up_val_weight, up_val_all, "columns"),
        own_copy(5, down_weight, down_all, "rows"),
    ]
    small = [
        (tokens, tokens_in),
        (mix_gain, mix_gain_in),
        (conv_taps, conv_taps_in),
        (chan_gain, chan_gain_in),
        (mix_post_gain, mix_post_gain_in),
        (ffn_gain, ffn_gain_in),
        (ffn_taps, ffn_taps_in),
        (ffn_post_gain, ffn_post_gain_in),
    ]
    loads = [
        pltpu.make_async_copy(source, held, load_sem.at[index])
        for index, (source, held) in enumerate(small)
    ]
    for copy in loads + own_copies:
        copy.start()

    glu_padded[:, 0:32, :] = jnp.zeros((glu_padded.shape[0], 32, LANES), F32)
    up_padded[:, :, 0:8, :] = jnp.zeros((2, up_padded.shape[1], 8, LANES), F32)
    own_rows = rows_at(member * rows, rows)

    def gain_of(held):
        return held[...].astype(F32).reshape(1, held.shape[0])

    loads[0].wait()
    loads[1].wait()
    mix_rows[own_rows] = rms_scale(tokens_in[...].astype(F32), gain_of(mix_gain_in)).astype(BF16)

    pl.semaphore_wait(barrier, len(friends) + w.inner.astype(jnp.int32))

    ahead = AHEAD
    for unit in range(ahead):
        stream.start(unit)
    mix_gather = RowGather(w, mix_rows, rows, group_rows, (mix_row_send, mix_row_recv))
    mix_gather.start(0)
    stream.events(list(range(len(pieces))), len(downs), ahead, ahead)
    stream.pump(9)
    mix_gather.relay(0)
    stream.pump(8)
    for unit in proj:
        stream.arrive(unit)
    own_copies[0].wait()
    own_copies[1].wait()
    mix_gather.finish(0)

    left = mix_rows[...]
    values = product(left, val_all[...].reshape(depth, local_ch))
    gate_sums = product(left, gate_all[...].reshape(depth, local_ch))
    glu = (values * jax.nn.sigmoid(gate_sums)).astype(BF16).astype(F32)
    for tile in range(mix_tiles):
        block = glu[:, tile * LANES : (tile + 1) * LANES].reshape(segments, LEN, LANES)
        glu_padded[tile * segments : (tile + 1) * segments, 32:, :] = block
    stream.pump(2)

    taps_count = conv_taps.shape[0]
    loads[2].wait()
    loads[3].wait()
    for tile in range(mix_tiles):
        lanes = rows_at(member * local_ch + tile * LANES, LANES, LANES)
        taps = conv_taps_in[:, lanes].astype(F32)

        @pl.loop(0, segments)
        def _(segment):
            total = jnp.zeros((LEN, LANES), F32)
            for k in range(taps_count):
                shifted = glu_padded[tile * segments + segment, pl.ds(33 - taps_count + k, LEN), :]
                total = total + shifted * taps[k : k + 1]
            conv_out[tile, rows_at(segment * LEN, LEN)] = total

        stream.pump(1)

    sums = conv_out[0]
    squares = conv_out[0] * conv_out[0]
    for tile in range(1, mix_tiles):
        sums = sums + conv_out[tile]
        squares = squares + conv_out[tile] * conv_out[tile]
    exact = lax.Precision.HIGHEST
    ones = jnp.ones((8, LANES), F32)
    contract_lanes = (((1,), (1,)), ((), ()))
    sums = lax.dot_general(ones, sums, contract_lanes, precision=exact, preferred_element_type=F32)
    squares = lax.dot_general(
        ones, squares, contract_lanes, precision=exact, preferred_element_type=F32
    )
    upper = lax.broadcasted_iota(jnp.int32, (8, group_rows), 0) < 4
    stats[0, :, :] = jnp.zeros(stats.shape[1:], F32)
    stats[0, :, 0:group_rows] = jnp.where(upper, sums, squares)

    def stat_copy(kind):
        device = (w.sibling, w.across, w.corner)[kind]
        return pltpu.make_async_remote_copy(
            src_ref=stats.at[0],
            dst_ref=stats.at[1 + kind],
            send_sem=stat_send.at[kind],
            recv_sem=stat_recv.at[kind],
            device_id={"tp": device},
        )

    for kind in (2, 1, 0):
        stat_copy(kind).start()
    stream.pump(3)
    for unit in outs:
        stream.arrive(unit)
    own_copies[2].wait()
    for kind in range(3):
        stat_copy(kind).wait_recv()
    total = stats[0] + stats[1] + stats[2] + stats[3]
    flipped = jnp.transpose(total)[:group_rows] / chan_gain.shape[0]
    chan_mean = flipped[:, 0:1]
    chan_var = flipped[:, 4:5] - chan_mean * chan_mean
    inverse = lax.rsqrt(chan_var + chan_epsilon)
    chan_gains = chan_gain_in[rows_at(member * local_ch, local_ch, LANES)].astype(F32)
    chan_gains = chan_gains.reshape(1, local_ch)
    for tile in range(mix_tiles):
        scaled = (conv_out[tile] - chan_mean) * inverse * chan_gains[:, tile * LANES : (tile + 1) * LANES]
        activated[:, tile * LANES : (tile + 1) * LANES] = jax.nn.silu(scaled).astype(BF16)

    mix_sum = RowScatter(
        w,
        1,
        rows,
        width * SUMS,
        mix_part,
        (mix_send0, mix_send1),
        (mix_recv0, mix_recv1),
        (mix_sum_send, mix_sum_recv),
        result,
    )
    places = [w.place]
    for near, far in ((3, 1), (1, 2), (2, 3)):
        places.append(jnp.where(w.inner, w.source(near), w.source(far)))
    for index in range(4 + 2):
        if index < 4:
            block = places[index]
            mix_sum.begin(block, product(activated[...], out_all[block]))
        if 1 <= index < 5:
            mix_sum.second(places[index - 1])
        if 2 <= index:
            mix_sum.third(places[index - 2])
        stream.pump(1)

    loads[4].wait()
    loads[5].wait()
    residual = tokens_in[...].astype(F32) + rms_scale(result[...], gain_of(mix_post_gain_in))
    residual = residual.astype(BF16)
    residual_ref[...] = residual
    ffn_rows[own_rows] = rms_scale(residual.astype(F32), gain_of(ffn_gain_in)).astype(BF16)
    ffn_gather = RowGather(w, ffn_rows, rows, group_rows, (ffn_row_send, ffn_row_recv))
    ffn_gather.start(0)
    ffn_gather.pair_copy().start()
    stream.pump(2)
    ffn_gather.relay(0)
    stream.pump(3)
    ffn_gather.pair_copy(incoming=True).wait_recv()
    ffn_gather.start(1)
    stream.pump(3)
    ffn_gather.relay(1)
    stream.pump_until(2 * len(downs))
    for unit in ups:
        stream.arrive(unit)
    own_copies[3].wait()
    own_copies[4].wait()
    loads[6].wait()

    def feed(level):
        ffn_gather.finish(level)
        left = ffn_rows[level * group_rows : (level + 1) * group_rows]
        for half, weight in enumerate((up_gate_all, up_val_all)):
            up = product(left, weight[...].reshape(depth, half_ff)).astype(BF16).astype(F32)
            for tile in range(ffn_tiles):
                block = up[:, tile * LANES : (tile + 1) * LANES].reshape(segments, LEN, LANES)
                up_padded[half, tile * segments : (tile + 1) * segments, 8:, :] = block
            stream.pump(1)
        for tile in range(ffn_tiles):
            first_lane = (2 * member + w.side) * half_ff + tile * LANES
            lanes = rows_at(first_lane, LANES, LANES)
            taps = [ffn_taps_in[:, half, lanes].astype(F32) for half in range(2)]

            @pl.loop(0, segments)
            def _(segment):
                convs = []
                for half in range(2):
                    conv = jnp.zeros((LEN, LANES), F32)
                    count = ffn_taps.shape[0]
                    for k in range(count):
                        shifted = up_padded[
                            half, tile * segments + segment, pl.ds(9 - count + k, LEN), :
                        ]
                        conv = conv + shifted * taps[half][k : k + 1]
                    convs.append(conv)
                value = jax.nn.gelu(convs[0], approximate=True) * convs[1]
                at = rows_at(level * group_rows + segment * LEN, LEN)
                hidden[at, tile * LANES : (tile + 1) * LANES] = value.astype(BF16)

    feed(0)
    feed(1)
    ffn_sum = RowScatter(
        w,
        2,
        rows,
        width,
        ffn_part,
        (ffn_send0, ffn_send1, ffn_send2),
        (ffn_recv0, ffn_recv1, ffn_recv2),
        (ffn_sum_send, ffn_sum_recv),
        result,
    )
    own_copies[5].wait()
    blocks = [(index, part) for index in range(4) for part in range(SUMS)]
    for step in range(len(blocks) + 2):
        if step < len(blocks):
            index, part = blocks[step]
            if index == 3:
                stream.pump_until(0)
            else:
                stream.pump(1)
            if index > 0:
                for role, slots in enumerate(((0, 3, 1, 2), (0, 1, 2, 3))):
                    chosen = jnp.logical_not(w.inner) if role else w.inner

                    @pl.when(chosen)
                    def _():
                        for unit in downs[2 * part : 2 * part + 2]:
                            stream.y_copy(unit, slots[index], incoming=True).wait_recv()

            right = down_all[places[index], :, part * width : (part + 1) * width]
            ffn_sum.begin(places[index] * SUMS + part, product(hidden[...], right))
        if 1 <= step < len(blocks) + 1:
            index, part = blocks[step - 1]
            ffn_sum.second(places[index] * SUMS + part)
        if 2 <= step:
            index, part = blocks[step - 2]
            ffn_sum.third(places[index] * SUMS + part)
    for index, part in blocks:
        ffn_sum.fourth(places[index] * SUMS + part)
    loads[7].wait()
    final = residual_ref[...].astype(F32) + rms_scale(result[...], gain_of(ffn_post_gain_in))
    out_staged[...] = final.astype(BF16)
    leave = pltpu.make_async_copy(out_staged, layer_out, load_sem.at[len(small)])
    leave.start()

    for unit in range(len(pieces)):
        stream.drain(unit)
    mix_gather.drain(0)
    ffn_gather.drain(0)
    ffn_gather.drain(1)
    ffn_gather.pair_copy().wait_send()
    for kind in range(3):
        stat_copy(kind).wait_send()
    for index in range(4):
        mix_sum.drain(index)
    for index in range(4 * SUMS):
        ffn_sum.drain(index)
    leave.wait()


def kernel_sizes(tokens, val_weight, out_weight, up_gate_weight, down_weight):
    rows = tokens.shape[0]
    return {
        "rows": rows,
        "group_rows": 4 * rows,
        "segments": 4 * rows // LEN,
        "depth": 4 * val_weight.shape[0],
        "local_ch": val_weight.shape[1],
        "half_ff": up_gate_weight.shape[1] // 2,
    }


def run_kernel(*args):
    (
        tokens,
        mix_gain,
        val_weight,
        gate_weight,
        conv_taps,
        chan_gain,
        out_weight,
        mix_post_gain,
        ffn_gain,
        up_gate_weight,
        up_val_weight,
        ffn_taps,
        down_weight,
        ffn_post_gain,
    ) = args
    sizes = kernel_sizes(tokens, val_weight, out_weight, up_gate_weight, down_weight)
    rows, group_rows, segments = sizes["rows"], sizes["group_rows"], sizes["segments"]
    local_ch, half_ff = sizes["local_ch"], sizes["half_ff"]
    width = out_weight.shape[1]
    model = tokens.shape[1]
    mix_tiles, ffn_tiles = local_ch // LANES, half_ff // LANES
    padded_rows = -(-group_rows // LANES) * LANES
    units = 6 + 2 * UP_CUTS + 2 * SUMS
    dma = pltpu.SemaphoreType.DMA
    shaped = [
        tokens,
        mix_gain,
        val_weight,
        gate_weight,
        conv_taps,
        chan_gain,
        out_weight,
        mix_post_gain,
        ffn_gain,
        up_gate_weight,
        up_val_weight,
        jnp.transpose(ffn_taps, (1, 0, 2)),
        down_weight,
        ffn_post_gain,
    ]
    scratch = [
        pltpu.VMEM(tokens.shape, BF16),
        pltpu.VMEM(conv_taps.shape, BF16),
        pltpu.VMEM(shaped[11].shape, BF16),
        pltpu.VMEM(mix_gain.shape, BF16),
        pltpu.VMEM(chan_gain.shape, BF16),
        pltpu.VMEM(mix_post_gain.shape, BF16),
        pltpu.VMEM(ffn_gain.shape, BF16),
        pltpu.VMEM(ffn_post_gain.shape, BF16),
        pltpu.VMEM((4, val_weight.shape[0], local_ch), BF16),
        pltpu.VMEM((4, gate_weight.shape[0], local_ch), BF16),
        pltpu.VMEM((4, local_ch, width), BF16),
        pltpu.VMEM((4, up_gate_weight.shape[0], half_ff), BF16),
        pltpu.VMEM((4, up_val_weight.shape[0], half_ff), BF16),
        pltpu.VMEM((4, half_ff, width), BF16),
        pltpu.VMEM((group_rows, model), BF16),
        pltpu.VMEM((2 * group_rows, model), BF16),
        pltpu.VMEM((mix_tiles * segments, 32 + LEN, LANES), F32),
        pltpu.VMEM((mix_tiles, group_rows, LANES), F32),
        pltpu.VMEM((4, 8, padded_rows), F32),
        pltpu.VMEM((group_rows, local_ch), BF16),
        pltpu.VMEM((2, ffn_tiles * segments, 8 + LEN, LANES), F32),
        pltpu.VMEM((2 * group_rows, half_ff), BF16),
        pltpu.VMEM((rows, model), BF16),
        pltpu.VMEM((rows, model), F32),
        pltpu.VMEM((4, 1, 2, 2, rows, width), F32),
        pltpu.VMEM((4 * SUMS, 2, 2, 2, rows, width // SUMS), F32),
        pltpu.VMEM((4, 1, 2, rows, width), BF16),
        pltpu.VMEM((4, 1, rows, width), BF16),
        pltpu.VMEM((4, 1, 2, rows, width), BF16),
        pltpu.VMEM((4, 1, rows, width), BF16),
        pltpu.VMEM((4 * SUMS, 2, 2, rows, width // SUMS), BF16),
        pltpu.VMEM((4 * SUMS, 2, rows, width // SUMS), BF16),
        pltpu.VMEM((4 * SUMS, rows, width // SUMS), BF16),
        pltpu.VMEM((4 * SUMS, 2, 2, rows, width // SUMS), BF16),
        pltpu.VMEM((4 * SUMS, 2, rows, width // SUMS), BF16),
        pltpu.VMEM((4 * SUMS, rows, width // SUMS), BF16),
        pltpu.VMEM(tokens.shape, BF16),
        dma((9,)),
        dma((6,)),
        dma((units, 4)),
        dma((units, 3)),
        dma((units, 3)),
        dma((units, 3)),
        dma((1, 3)),
        dma((1, 3)),
        dma((2, 4)),
        dma((2, 4)),
        dma((3,)),
        dma((3,)),
        dma((2, 4)),
        dma((2, 4)),
        dma((3, 4 * SUMS)),
        dma((3, 4 * SUMS)),
    ]
    return pl.pallas_call(
        functools.partial(layer_kernel, sizes),
        out_shape=jax.ShapeDtypeStruct(tokens.shape, BF16),
        in_specs=[pl.BlockSpec(memory_space=pltpu.HBM)] * len(shaped),
        out_specs=pl.BlockSpec(memory_space=pl.ANY),
        scratch_shapes=scratch,
        compiler_params=pltpu.CompilerParams(
            collective_id=0, has_side_effects=True, vmem_limit_bytes=67_043_328
        ),
    )(*shaped)


def fits(mesh, args):
    tokens, val_weight, out_weight = args[0], args[2], args[6]
    up_gate_weight, down_weight = args[9], args[12]
    if (mesh.shape["grp"], mesh.shape["fs"], mesh.shape["tp"]) != (2, 4, 4):
        return False
    rows = tokens.shape[0] // 32
    local_ch, local_ff = val_weight.shape[1] // 4, up_gate_weight.shape[1] // 4
    local_model = tokens.shape[1] // 4
    return (
        rows % 16 == 0
        and local_model % (32 * UP_CUTS) == 0
        and local_ff % 128 == 0
        and 4 * rows % LEN == 0
        and local_ch % LANES == 0
        and local_ff % (2 * LANES) == 0
        and local_model % (SUMS * LANES) == 0
        and args[4].shape[0] <= 32
        and args[11].shape[1] <= 8
    )


def solution(mesh):
    specs = (
        P(("grp", "fs", "tp"), None),
        P(),
        P("fs", "tp"),
        P("fs", "tp"),
        P(),
        P(),
        P("tp", "fs"),
        P(),
        P(),
        P("fs", "tp"),
        P("fs", "tp"),
        P(),
        P("tp", "fs"),
        P(),
    )

    def whole(*args):
        body = run_kernel if fits(mesh, args) else plain
        step = jax.shard_map(
            body,
            mesh=mesh,
            in_specs=specs,
            out_specs=P(("grp", "fs", "tp"), None),
            check_vma=False,
        )
        return step(*args)

    return whole
```

```python
import functools

import jax
import jax.numpy as jnp
from jax import lax
from jax.experimental import pallas as pl
from jax.experimental.pallas import tpu as pltpu
from jax.sharding import PartitionSpec as P

LEN = 64
LANES = 128
SUMS = 1
UP_CUTS = 4
AHEAD = 2
F32 = jnp.float32
BF16 = jnp.bfloat16

norm_epsilon = 1e-06
chan_epsilon = 1e-05


def rms_scale(values, gain):
    inverse = lax.rsqrt(jnp.mean(values * values, axis=-1, keepdims=True) + norm_epsilon)
    return values * inverse * gain.astype(F32)


def depthwise(signal, tap_table):
    taps_count = tap_table.shape[0]
    channels = signal.shape[1]
    shaped = signal.astype(F32).reshape(signal.shape[0] // LEN, LEN, channels)
    padded = jnp.pad(shaped, ((0, 0), (taps_count - 1, 0), (0, 0)))
    tap_values = tap_table.astype(F32)
    result = jnp.zeros(shaped.shape, F32)
    for offset in range(taps_count):
        result = result + padded[:, offset : offset + LEN, :] * tap_values[offset]
    return result.reshape(signal.shape[0], channels)


def gather_rows(weight):
    return lax.all_gather(weight, "fs", axis=0, tiled=True)


def gather_columns(weight):
    return lax.all_gather(weight, "fs", axis=1, tiled=True)


def product(left, right):
    return jnp.dot(left, right, preferred_element_type=F32)


def scatter_sum(part):
    return lax.psum_scatter(
        part.astype(BF16), "tp", scatter_dimension=0, tiled=True
    ).astype(F32)


def plain(
    tokens,
    mix_gain,
    val_weight,
    gate_weight,
    conv_taps,
    chan_gain,
    out_weight,
    mix_post_gain,
    ffn_gain,
    up_gate_weight,
    up_val_weight,
    ffn_taps,
    down_weight,
    ffn_post_gain,
):
    member = lax.axis_index("tp")
    normed_own = rms_scale(tokens.astype(F32), mix_gain).astype(BF16)
    normed = lax.all_gather(normed_own, "tp", axis=0, tiled=True)
    local_ch = val_weight.shape[1]
    values = product(normed, gather_rows(val_weight))
    gate_sums = product(normed, gather_rows(gate_weight))
    glu_out = (values * jax.nn.sigmoid(gate_sums)).astype(BF16)
    own_taps = lax.dynamic_slice_in_dim(conv_taps, member * local_ch, local_ch, 1)
    conv_out = depthwise(glu_out, own_taps)
    totals, squares = lax.psum(
        (jnp.sum(conv_out, axis=1), jnp.sum(conv_out * conv_out, axis=1)), "tp"
    )
    all_channels = chan_gain.shape[0]
    chan_mean = totals[:, None] / all_channels
    chan_var = squares[:, None] / all_channels - chan_mean * chan_mean
    own_gain = lax.dynamic_slice_in_dim(chan_gain, member * local_ch, local_ch, 0).astype(F32)
    activated = jax.nn.silu((conv_out - chan_mean) * lax.rsqrt(chan_var + chan_epsilon) * own_gain)
    mixed_sum = scatter_sum(product(activated.astype(BF16), gather_columns(out_weight)))
    residual = (tokens.astype(F32) + rms_scale(mixed_sum, mix_post_gain)).astype(BF16)
    normed_share = rms_scale(residual.astype(F32), ffn_gain).astype(BF16)
    normed_ffn = lax.all_gather(normed_share, "tp", axis=0, tiled=True)
    local_ff = up_gate_weight.shape[1]
    own_ffn_taps = lax.dynamic_slice_in_dim(ffn_taps, member * local_ff, local_ff, 2)
    up_gate = product(normed_ffn, gather_rows(up_gate_weight)).astype(BF16)
    up_val = product(normed_ffn, gather_rows(up_val_weight)).astype(BF16)
    gate_conv = depthwise(up_gate, own_ffn_taps[0])
    val_conv = depthwise(up_val, own_ffn_taps[1])
    hidden = (jax.nn.gelu(gate_conv, approximate=True) * val_conv).astype(BF16)
    ffn_sum = scatter_sum(product(hidden, gather_columns(down_weight)))
    return (residual.astype(F32) + rms_scale(ffn_sum, ffn_post_gain)).astype(BF16)


def rows_at(start, size, unit=16):
    return pl.ds(pl.multiple_of(start, unit), size)


class Where:
    def __init__(self):
        self.place = lax.axis_index("fs")
        self.half = lax.axis_index("grp")
        self.member = lax.axis_index("tp")
        place, member = self.place, self.member
        self.side = place // 2
        self.inner = jnp.logical_or(place == 1, place == 2)
        self.chip = member // 2
        self.core = member % 2
        self.mate = place + 1 - 2 * (place % 2)
        self.over = 2 - self.side
        self.pair = lax.rem(place + 2, 4)
        self.sibling = member + 1 - 2 * self.core
        self.across = lax.rem(member + 2, 4)
        self.corner = self.sibling + 2 - 4 * self.chip

    def source(self, slot):
        if slot == 1:
            return self.mate
        if slot == 2:
            return self.pair
        return self.pair + 1 - 2 * (self.place % 2)


class Piece:
    def __init__(self, source, held, start, size, stride, sided, columns, lanes=None):
        self.source_ref = source
        self.held = held
        self.start = start
        self.size = size
        self.stride = stride
        self.sided = sided
        self.columns = columns
        self.lanes = lanes

    def read(self, where, side):
        first = where.half * self.stride + self.start
        if self.sided == "rows":
            first = side * (2 * self.stride) + first
        rows = rows_at(first, self.size)
        if self.sided == "columns":
            columns = rows_at(side * self.columns, self.columns, LANES)
            return self.source_ref.at[rows, columns]
        if self.lanes is not None:
            return self.source_ref.at[rows, self.lanes]
        return self.source_ref.at[rows]

    def target(self, where, origin, half):
        first = half * self.stride + self.start
        rows = rows_at(first, self.size)
        if self.lanes is not None:
            return self.held.at[origin, rows, self.lanes]
        return self.held.at[origin, rows]


class Stream:
    def __init__(self, where, pieces, semaphores):
        self.where = where
        self.pieces = pieces
        self.z_send, self.z_recv, self.y_send, self.y_recv = semaphores

    def z_copy(self, unit, kind):
        w, piece = self.where, self.pieces[unit]
        if kind < 2:
            side = w.side if kind == 0 else 1 - w.side
            source = piece.read(w, side)
            target = piece.target(w, w.place, w.half)
            device = w.mate if kind == 0 else w.over
            if kind == 0:
                slot = 1
            else:
                slot = 2 + w.inner.astype(jnp.int32)
        else:
            target = piece.target(w, w.source(kind), w.half)
            source = target
            device = w.mate
            slot = 5 - kind
        return pltpu.make_async_remote_copy(
            src_ref=source,
            dst_ref=target,
            send_sem=self.z_send.at[unit, kind],
            recv_sem=self.z_recv.at[unit, slot - 1],
            device_id={"fs": device},
        )

    def z_arrival(self, unit, slot):
        w = self.where
        target = self.pieces[unit].target(w, w.source(slot), w.half)
        return pltpu.make_async_remote_copy(
            src_ref=target,
            dst_ref=target,
            send_sem=self.z_send.at[unit, 0],
            recv_sem=self.z_recv.at[unit, slot - 1],
            device_id={"fs": w.mate},
        )

    def y_copy(self, unit, slot, incoming=False):
        w = self.where
        half = 1 - w.half if incoming else w.half
        target = self.pieces[unit].target(w, w.source(slot), half)
        return pltpu.make_async_remote_copy(
            src_ref=target,
            dst_ref=target,
            send_sem=self.y_send.at[unit, slot - 1],
            recv_sem=self.y_recv.at[unit, slot - 1],
            device_id={"grp": 1 - w.half},
        )

    def start(self, unit):
        self.z_copy(unit, 0).start()
        self.z_copy(unit, 1).start()

    def serve(self, unit, slot, relay):
        self.z_arrival(unit, slot).wait_recv()
        if relay:
            self.z_copy(unit, slot).start()
        self.y_copy(unit, slot).start()

    def events(self, order, tail, ahead, lag):
        count, body = len(order), len(order) - tail
        inner, outer = [], []
        for index in range(count + lag):
            first = [order[index + ahead]] if index + ahead < count else []
            if index == body - 1:
                first = order[index + ahead :]
            elif index >= body:
                first = []
            if index < body:
                inner.append((first, order[index], 2, True))
                inner.append(([], order[index], 3, True))
                inner.append(([], order[index], 1, False))
            if index < count:
                outer.append((first, order[index], 1, False))
            if lag <= index < body + lag:
                outer.append(([], order[index - lag], 3, False))
                outer.append(([], order[index - lag], 2, False))
        last = order[body:]
        for slot in (3, 1, 2):
            inner += [([], unit, slot, slot > 1) for unit in last]
        for slot in (2, 3):
            outer += [([], unit, slot, False) for unit in last]
        self.waiting = list(zip(inner, outer))

    def pump_until(self, left):
        self.pump(max(0, len(self.waiting) - left))

    def pump(self, count):
        for _ in range(min(count, len(self.waiting))):
            pair = self.waiting.pop(0)
            for role, (begin, unit, slot, relay) in enumerate(pair):
                chosen = jnp.logical_not(self.where.inner) if role else self.where.inner

                @pl.when(chosen)
                def _():
                    for other in begin:
                        self.start(other)
                    self.serve(unit, slot, relay)

    def arrive(self, unit):
        for slot in (1, 3, 2):
            self.y_copy(unit, slot, incoming=True).wait_recv()

    def drain(self, unit):
        self.z_copy(unit, 0).wait_send()
        self.z_copy(unit, 1).wait_send()
        for slot in (1, 2, 3):
            if slot > 1:

                @pl.when(self.where.inner)
                def _():
                    self.z_copy(unit, slot).wait_send()

            self.y_copy(unit, slot).wait_send()


class RowGather:
    def __init__(self, where, held, rows, group_rows, semaphores):
        self.where = where
        self.held = held
        self.rows = rows
        self.group_rows = group_rows
        self.send, self.recv = semaphores

    def view(self, level, member):
        first = level * self.group_rows + member * self.rows
        return self.held.at[rows_at(first, self.rows)]

    def copy(self, level, kind):
        w = self.where
        view = self.view(level, w.across if kind == 2 else w.member)
        return pltpu.make_async_remote_copy(
            src_ref=view,
            dst_ref=view,
            send_sem=self.send.at[level, kind],
            recv_sem=self.recv.at[level, kind],
            device_id={"tp": w.across if kind == 1 else w.sibling},
        )

    def arrival(self, level, kind):
        w = self.where
        member = (w.sibling, w.across, w.corner)[kind]
        view = self.view(level, member)
        return pltpu.make_async_remote_copy(
            src_ref=view,
            dst_ref=view,
            send_sem=self.send.at[level, kind],
            recv_sem=self.recv.at[level, kind],
            device_id={"tp": w.across if kind == 1 else w.sibling},
        )

    def start(self, level):
        self.copy(level, 1).start()
        self.copy(level, 0).start()

    def relay(self, level):
        self.arrival(level, 1).wait_recv()
        self.copy(level, 2).start()

    def finish(self, level):
        self.arrival(level, 0).wait_recv()
        self.arrival(level, 2).wait_recv()

    def drain(self, level):
        for kind in range(3):
            self.copy(level, kind).wait_send()

    def pair_copy(self, incoming=False):
        w = self.where
        mine = self.view(0, w.member)
        other = self.view(1, w.member)
        return pltpu.make_async_remote_copy(
            src_ref=other if incoming else mine,
            dst_ref=other,
            send_sem=self.send.at[1, 3],
            recv_sem=self.recv.at[1, 3],
            device_id={"fs": w.pair},
        )


class RowScatter:
    def __init__(self, where, levels, rows, width, part, sends, recvs, semaphores, result):
        self.where = where
        self.levels = levels
        self.rows = rows
        self.width = width
        self.part = part
        self.sends = sends
        self.recvs = recvs
        self.send_sem, self.recv_sem = semaphores
        self.result = result

    def copy(self, block, stage):
        w = self.where
        device = ({"tp": w.sibling}, {"tp": w.across}, {"fs": w.pair})[stage]
        return pltpu.make_async_remote_copy(
            src_ref=self.sends[stage].at[block],
            dst_ref=self.recvs[stage].at[block],
            send_sem=self.send_sem.at[stage, block],
            recv_sem=self.recv_sem.at[stage, block],
            device_id=device,
        )

    def begin(self, block, value):
        w = self.where
        shape = (self.levels, 2, 2, self.rows, self.width)
        self.part[block] = value.reshape(shape)
        self.sends[0][block] = self.part[block, :, :, 1 - w.core].astype(BF16)
        self.copy(block, 0).start()

    def second(self, block):
        w = self.where
        self.copy(block, 0).wait_recv()
        away = self.part[block, :, 1 - w.chip, w.core]
        away = away + self.recvs[0][block, :, 1 - w.chip].astype(F32)
        self.sends[1][block] = away.astype(BF16)
        self.copy(block, 1).start()
        kept = self.part[block, :, w.chip, w.core]
        kept = kept + self.recvs[0][block, :, w.chip].astype(F32)
        self.part[block, :, 0, 0] = kept

    def third(self, block):
        self.copy(block, 1).wait_recv()
        if self.levels > 1:
            away = self.part[block, 1, 0, 0] + self.recvs[1][block, 1].astype(F32)
            self.sends[2][block] = away.astype(BF16)
            self.copy(block, 2).start()
            kept = self.part[block, 0, 0, 0] + self.recvs[1][block, 0].astype(F32)
            self.part[block, 0, 0, 0] = kept
        else:
            self.store(block, self.part[block, 0, 0, 0] + self.recvs[1][block, 0].astype(F32))

    def fourth(self, block):
        self.copy(block, 2).wait_recv()
        self.store(block, self.part[block, 0, 0, 0] + self.recvs[2][block].astype(F32))

    def store(self, block, value):
        self.result[:, rows_at(block * self.width, self.width, LANES)] = value

    def drain(self, block):
        for stage in range(1 + self.levels):
            self.copy(block, stage).wait_send()


def layer_kernel(sizes, *refs):
    (
        tokens,
        mix_gain,
        val_weight,
        gate_weight,
        conv_taps,
        chan_gain,
        out_weight,
        mix_post_gain,
        ffn_gain,
        up_gate_weight,
        up_val_weight,
        ffn_taps,
        down_weight,
        ffn_post_gain,
        layer_out,
        tokens_in,
        conv_taps_in,
        ffn_taps_in,
        mix_gain_in,
        chan_gain_in,
        mix_post_gain_in,
        ffn_gain_in,
        ffn_post_gain_in,
        val_all,
        gate_all,
        out_all,
        up_gate_all,
        up_val_all,
        down_all,
        mix_rows,
        ffn_rows,
        glu_padded,
        conv_out,
        stats,
        activated,
        up_padded,
        hidden,
        residual_ref,
        result,
        mix_part,
        ffn_part,
        mix_send0,
        mix_send1,
        mix_recv0,
        mix_recv1,
        ffn_send0,
        ffn_send1,
        ffn_send2,
        ffn_recv0,
        ffn_recv1,
        ffn_recv2,
        out_staged,
        load_sem,
        own_sem,
        z_send,
        z_recv,
        y_send,
        y_recv,
        mix_row_send,
        mix_row_recv,
        ffn_row_send,
        ffn_row_recv,
        stat_send,
        stat_recv,
        mix_sum_send,
        mix_sum_recv,
        ffn_sum_send,
        ffn_sum_recv,
    ) = refs
    w = Where()
    rows, group_rows, segments = sizes["rows"], sizes["group_rows"], sizes["segments"]
    depth, local_ch, half_ff = sizes["depth"], sizes["local_ch"], sizes["half_ff"]
    width = out_all.shape[2] // SUMS
    mix_tiles, ffn_tiles = local_ch // LANES, half_ff // LANES
    member = w.member

    barrier = pltpu.get_barrier_semaphore()
    friends = [
        {"tp": w.sibling},
        {"tp": w.across},
        {"tp": w.corner},
        {"grp": 1 - w.half},
        {"fs": w.mate},
        {"fs": w.pair},
    ]
    for friend in friends:
        pl.semaphore_signal(barrier, inc=1, device_id=friend)

    @pl.when(w.inner)
    def _():
        pl.semaphore_signal(barrier, inc=1, device_id={"fs": 3 - w.place})

    pieces = []

    def cut(source, held, sided, chunks):
        total = held.shape[1] // 2
        size = total // chunks
        return [
            Piece(source, held, index * size, size, total, sided, held.shape[2])
            for index in range(chunks)
        ]

    val_pieces = cut(val_weight, val_all, None, 2)
    gate_pieces = cut(gate_weight, gate_all, None, 2)
    out_pieces = cut(out_weight, out_all, None, 2)
    up_gate_pieces = cut(up_gate_weight, up_gate_all, "columns", UP_CUTS)
    up_val_pieces = cut(up_val_weight, up_val_all, "columns", UP_CUTS)
    down_rows = half_ff // 2
    down_size = down_rows // 2
    down_pieces = [
        Piece(
            down_weight,
            down_all,
            row * down_size,
            down_size,
            down_rows,
            "rows",
            None,
            pl.ds(part * width, width),
        )
        for part in range(SUMS)
        for row in range(2)
    ]
    mixed = [piece for pair in zip(val_pieces, gate_pieces) for piece in pair]
    upward = [piece for pair in zip(up_gate_pieces, up_val_pieces) for piece in pair]
    pieces = mixed + out_pieces + upward + down_pieces
    proj = list(range(0, 4))
    outs = list(range(4, 6))
    ups = list(range(6, 6 + len(upward)))
    downs = list(range(6 + len(upward), len(pieces)))
    stream = Stream(w, pieces, (z_send, z_recv, y_send, y_recv))

    def own_copy(index, source, held, sided):
        if sided == "columns":
            view = source.at[:, rows_at(w.side * held.shape[2], held.shape[2], LANES)]
        elif sided == "rows":
            view = source.at[rows_at(w.side * held.shape[1], held.shape[1])]
        else:
            view = source
        return pltpu.make_async_copy(view, held.at[w.place], own_sem.at[index])

    own_copies = [
        own_copy(0, val_weight, val_all, None),
        own_copy(1, gate_weight, gate_all, None),
        own_copy(2, out_weight, out_all, None),
        own_copy(3, up_gate_weight, up_gate_all, "columns"),
        own_copy(4, up_val_weight, up_val_all, "columns"),
        own_copy(5, down_weight, down_all, "rows"),
    ]
    small = [
        (tokens, tokens_in),
        (mix_gain, mix_gain_in),
        (conv_taps, conv_taps_in),
        (chan_gain, chan_gain_in),
        (mix_post_gain, mix_post_gain_in),
        (ffn_gain, ffn_gain_in),
        (ffn_taps, ffn_taps_in),
        (ffn_post_gain, ffn_post_gain_in),
    ]
    loads = [
        pltpu.make_async_copy(source, held, load_sem.at[index])
        for index, (source, held) in enumerate(small)
    ]
    for copy in loads + own_copies:
        copy.start()

    glu_padded[:, 0:32, :] = jnp.zeros((glu_padded.shape[0], 32, LANES), F32)
    up_padded[:, :, 0:8, :] = jnp.zeros((2, up_padded.shape[1], 8, LANES), F32)
    own_rows = rows_at(member * rows, rows)

    def gain_of(held):
        return held[...].astype(F32).reshape(1, held.shape[0])

    pl.semaphore_wait(barrier, len(friends) + w.inner.astype(jnp.int32))

    ahead = AHEAD
    for unit in range(ahead):
        stream.start(unit)
    loads[0].wait()
    loads[1].wait()
    mix_rows[own_rows] = rms_scale(tokens_in[...].astype(F32), gain_of(mix_gain_in)).astype(BF16)
    mix_gather = RowGather(w, mix_rows, rows, group_rows, (mix_row_send, mix_row_recv))
    mix_gather.start(0)
    stream.events(list(range(len(pieces))), len(downs), ahead, ahead)
    stream.pump(9)
    mix_gather.relay(0)
    stream.pump(8)
    for unit in proj:
        stream.arrive(unit)
    own_copies[0].wait()
    own_copies[1].wait()
    mix_gather.finish(0)

    left = mix_rows[...]
    values = product(left, val_all[...].reshape(depth, local_ch))
    gate_sums = product(left, gate_all[...].reshape(depth, local_ch))
    glu = (values * jax.nn.sigmoid(gate_sums)).astype(BF16).astype(F32)
    for tile in range(mix_tiles):
        block = glu[:, tile * LANES : (tile + 1) * LANES].reshape(segments, LEN, LANES)
        glu_padded[tile * segments : (tile + 1) * segments, 32:, :] = block
    stream.pump(2)

    taps_count = conv_taps.shape[0]
    loads[2].wait()
    loads[3].wait()
    for tile in range(mix_tiles):
        lanes = rows_at(member * local_ch + tile * LANES, LANES, LANES)
        taps = conv_taps_in[:, lanes].astype(F32)

        @pl.loop(0, segments)
        def _(segment):
            total = jnp.zeros((LEN, LANES), F32)
            for k in range(taps_count):
                shifted = glu_padded[tile * segments + segment, pl.ds(33 - taps_count + k, LEN), :]
                total = total + shifted * taps[k : k + 1]
            conv_out[tile, rows_at(segment * LEN, LEN)] = total

        stream.pump(1)

    sums = conv_out[0]
    squares = conv_out[0] * conv_out[0]
    for tile in range(1, mix_tiles):
        sums = sums + conv_out[tile]
        squares = squares + conv_out[tile] * conv_out[tile]
    exact = lax.Precision.HIGHEST
    ones = jnp.ones((8, LANES), F32)
    contract_lanes = (((1,), (1,)), ((), ()))
    sums = lax.dot_general(ones, sums, contract_lanes, precision=exact, preferred_element_type=F32)
    squares = lax.dot_general(
        ones, squares, contract_lanes, precision=exact, preferred_element_type=F32
    )
    upper = lax.broadcasted_iota(jnp.int32, (8, group_rows), 0) < 4
    stats[0, :, :] = jnp.zeros(stats.shape[1:], F32)
    stats[0, :, 0:group_rows] = jnp.where(upper, sums, squares)

    def stat_copy(kind):
        device = (w.sibling, w.across, w.corner)[kind]
        return pltpu.make_async_remote_copy(
            src_ref=stats.at[0],
            dst_ref=stats.at[1 + kind],
            send_sem=stat_send.at[kind],
            recv_sem=stat_recv.at[kind],
            device_id={"tp": device},
        )

    for kind in (2, 1, 0):
        stat_copy(kind).start()
    stream.pump(3)
    for unit in outs:
        stream.arrive(unit)
    own_copies[2].wait()
    for kind in range(3):
        stat_copy(kind).wait_recv()
    total = stats[0] + stats[1] + stats[2] + stats[3]
    flipped = jnp.transpose(total)[:group_rows] / chan_gain.shape[0]
    chan_mean = flipped[:, 0:1]
    chan_var = flipped[:, 4:5] - chan_mean * chan_mean
    inverse = lax.rsqrt(chan_var + chan_epsilon)
    chan_gains = chan_gain_in[rows_at(member * local_ch, local_ch, LANES)].astype(F32)
    chan_gains = chan_gains.reshape(1, local_ch)
    for tile in range(mix_tiles):
        scaled = (conv_out[tile] - chan_mean) * inverse * chan_gains[:, tile * LANES : (tile + 1) * LANES]
        activated[:, tile * LANES : (tile + 1) * LANES] = jax.nn.silu(scaled).astype(BF16)

    mix_sum = RowScatter(
        w,
        1,
        rows,
        width * SUMS,
        mix_part,
        (mix_send0, mix_send1),
        (mix_recv0, mix_recv1),
        (mix_sum_send, mix_sum_recv),
        result,
    )
    places = [w.place]
    for near, far in ((3, 1), (1, 2), (2, 3)):
        places.append(jnp.where(w.inner, w.source(near), w.source(far)))
    for index in range(4 + 2):
        if index < 4:
            block = places[index]
            mix_sum.begin(block, product(activated[...], out_all[block]))
        if 1 <= index < 5:
            mix_sum.second(places[index - 1])
        if 2 <= index:
            mix_sum.third(places[index - 2])
        stream.pump(1)

    loads[4].wait()
    loads[5].wait()
    residual = tokens_in[...].astype(F32) + rms_scale(result[...], gain_of(mix_post_gain_in))
    residual = residual.astype(BF16)
    residual_ref[...] = residual
    ffn_rows[own_rows] = rms_scale(residual.astype(F32), gain_of(ffn_gain_in)).astype(BF16)
    ffn_gather = RowGather(w, ffn_rows, rows, group_rows, (ffn_row_send, ffn_row_recv))
    ffn_gather.start(0)
    ffn_gather.pair_copy().start()
    stream.pump(2)
    ffn_gather.relay(0)
    stream.pump(3)
    ffn_gather.pair_copy(incoming=True).wait_recv()
    ffn_gather.start(1)
    stream.pump(3)
    ffn_gather.relay(1)
    stream.pump_until(2 * len(downs))
    for unit in ups:
        stream.arrive(unit)
    own_copies[3].wait()
    own_copies[4].wait()
    loads[6].wait()

    def feed(level):
        ffn_gather.finish(level)
        left = ffn_rows[level * group_rows : (level + 1) * group_rows]
        for half, weight in enumerate((up_gate_all, up_val_all)):
            up = product(left, weight[...].reshape(depth, half_ff)).astype(BF16).astype(F32)
            for tile in range(ffn_tiles):
                block = up[:, tile * LANES : (tile + 1) * LANES].reshape(segments, LEN, LANES)
                up_padded[half, tile * segments : (tile + 1) * segments, 8:, :] = block
            stream.pump(1)
        for tile in range(ffn_tiles):
            first_lane = (2 * member + w.side) * half_ff + tile * LANES
            lanes = rows_at(first_lane, LANES, LANES)
            taps = [ffn_taps_in[:, half, lanes].astype(F32) for half in range(2)]

            @pl.loop(0, segments)
            def _(segment):
                convs = []
                for half in range(2):
                    conv = jnp.zeros((LEN, LANES), F32)
                    count = ffn_taps.shape[0]
                    for k in range(count):
                        shifted = up_padded[
                            half, tile * segments + segment, pl.ds(9 - count + k, LEN), :
                        ]
                        conv = conv + shifted * taps[half][k : k + 1]
                    convs.append(conv)
                value = jax.nn.gelu(convs[0], approximate=True) * convs[1]
                at = rows_at(level * group_rows + segment * LEN, LEN)
                hidden[at, tile * LANES : (tile + 1) * LANES] = value.astype(BF16)

    feed(0)
    feed(1)
    ffn_sum = RowScatter(
        w,
        2,
        rows,
        width,
        ffn_part,
        (ffn_send0, ffn_send1, ffn_send2),
        (ffn_recv0, ffn_recv1, ffn_recv2),
        (ffn_sum_send, ffn_sum_recv),
        result,
    )
    own_copies[5].wait()
    blocks = [(index, part) for index in range(4) for part in range(SUMS)]
    for step in range(len(blocks) + 2):
        if step < len(blocks):
            index, part = blocks[step]
            if index == 3:
                stream.pump_until(0)
            else:
                stream.pump(1)
            if index > 0:
                for role, slots in enumerate(((0, 3, 1, 2), (0, 1, 2, 3))):
                    chosen = jnp.logical_not(w.inner) if role else w.inner

                    @pl.when(chosen)
                    def _():
                        for unit in downs[2 * part : 2 * part + 2]:
                            stream.y_copy(unit, slots[index], incoming=True).wait_recv()

            right = down_all[places[index], :, part * width : (part + 1) * width]
            ffn_sum.begin(places[index] * SUMS + part, product(hidden[...], right))
        if 1 <= step < len(blocks) + 1:
            index, part = blocks[step - 1]
            ffn_sum.second(places[index] * SUMS + part)
        if 2 <= step:
            index, part = blocks[step - 2]
            ffn_sum.third(places[index] * SUMS + part)
    for index, part in blocks:
        ffn_sum.fourth(places[index] * SUMS + part)
    loads[7].wait()
    final = residual_ref[...].astype(F32) + rms_scale(result[...], gain_of(ffn_post_gain_in))
    out_staged[...] = final.astype(BF16)
    leave = pltpu.make_async_copy(out_staged, layer_out, load_sem.at[len(small)])
    leave.start()

    for unit in range(len(pieces)):
        stream.drain(unit)
    mix_gather.drain(0)
    ffn_gather.drain(0)
    ffn_gather.drain(1)
    ffn_gather.pair_copy().wait_send()
    for kind in range(3):
        stat_copy(kind).wait_send()
    for index in range(4):
        mix_sum.drain(index)
    for index in range(4 * SUMS):
        ffn_sum.drain(index)
    leave.wait()


def kernel_sizes(tokens, val_weight, out_weight, up_gate_weight, down_weight):
    rows = tokens.shape[0]
    return {
        "rows": rows,
        "group_rows": 4 * rows,
        "segments": 4 * rows // LEN,
        "depth": 4 * val_weight.shape[0],
        "local_ch": val_weight.shape[1],
        "half_ff": up_gate_weight.shape[1] // 2,
    }


def run_kernel(*args):
    (
        tokens,
        mix_gain,
        val_weight,
        gate_weight,
        conv_taps,
        chan_gain,
        out_weight,
        mix_post_gain,
        ffn_gain,
        up_gate_weight,
        up_val_weight,
        ffn_taps,
        down_weight,
        ffn_post_gain,
    ) = args
    sizes = kernel_sizes(tokens, val_weight, out_weight, up_gate_weight, down_weight)
    rows, group_rows, segments = sizes["rows"], sizes["group_rows"], sizes["segments"]
    local_ch, half_ff = sizes["local_ch"], sizes["half_ff"]
    width = out_weight.shape[1]
    model = tokens.shape[1]
    mix_tiles, ffn_tiles = local_ch // LANES, half_ff // LANES
    padded_rows = -(-group_rows // LANES) * LANES
    units = 6 + 2 * UP_CUTS + 2 * SUMS
    dma = pltpu.SemaphoreType.DMA
    shaped = [
        tokens,
        mix_gain,
        val_weight,
        gate_weight,
        conv_taps,
        chan_gain,
        out_weight,
        mix_post_gain,
        ffn_gain,
        up_gate_weight,
        up_val_weight,
        jnp.transpose(ffn_taps, (1, 0, 2)),
        down_weight,
        ffn_post_gain,
    ]
    scratch = [
        pltpu.VMEM(tokens.shape, BF16),
        pltpu.VMEM(conv_taps.shape, BF16),
        pltpu.VMEM(shaped[11].shape, BF16),
        pltpu.VMEM(mix_gain.shape, BF16),
        pltpu.VMEM(chan_gain.shape, BF16),
        pltpu.VMEM(mix_post_gain.shape, BF16),
        pltpu.VMEM(ffn_gain.shape, BF16),
        pltpu.VMEM(ffn_post_gain.shape, BF16),
        pltpu.VMEM((4, val_weight.shape[0], local_ch), BF16),
        pltpu.VMEM((4, gate_weight.shape[0], local_ch), BF16),
        pltpu.VMEM((4, local_ch, width), BF16),
        pltpu.VMEM((4, up_gate_weight.shape[0], half_ff), BF16),
        pltpu.VMEM((4, up_val_weight.shape[0], half_ff), BF16),
        pltpu.VMEM((4, half_ff, width), BF16),
        pltpu.VMEM((group_rows, model), BF16),
        pltpu.VMEM((2 * group_rows, model), BF16),
        pltpu.VMEM((mix_tiles * segments, 32 + LEN, LANES), F32),
        pltpu.VMEM((mix_tiles, group_rows, LANES), F32),
        pltpu.VMEM((4, 8, padded_rows), F32),
        pltpu.VMEM((group_rows, local_ch), BF16),
        pltpu.VMEM((2, ffn_tiles * segments, 8 + LEN, LANES), F32),
        pltpu.VMEM((2 * group_rows, half_ff), BF16),
        pltpu.VMEM((rows, model), BF16),
        pltpu.VMEM((rows, model), F32),
        pltpu.VMEM((4, 1, 2, 2, rows, width), F32),
        pltpu.VMEM((4 * SUMS, 2, 2, 2, rows, width // SUMS), F32),
        pltpu.VMEM((4, 1, 2, rows, width), BF16),
        pltpu.VMEM((4, 1, rows, width), BF16),
        pltpu.VMEM((4, 1, 2, rows, width), BF16),
        pltpu.VMEM((4, 1, rows, width), BF16),
        pltpu.VMEM((4 * SUMS, 2, 2, rows, width // SUMS), BF16),
        pltpu.VMEM((4 * SUMS, 2, rows, width // SUMS), BF16),
        pltpu.VMEM((4 * SUMS, rows, width // SUMS), BF16),
        pltpu.VMEM((4 * SUMS, 2, 2, rows, width // SUMS), BF16),
        pltpu.VMEM((4 * SUMS, 2, rows, width // SUMS), BF16),
        pltpu.VMEM((4 * SUMS, rows, width // SUMS), BF16),
        pltpu.VMEM(tokens.shape, BF16),
        dma((9,)),
        dma((6,)),
        dma((units, 4)),
        dma((units, 3)),
        dma((units, 3)),
        dma((units, 3)),
        dma((1, 3)),
        dma((1, 3)),
        dma((2, 4)),
        dma((2, 4)),
        dma((3,)),
        dma((3,)),
        dma((2, 4)),
        dma((2, 4)),
        dma((3, 4 * SUMS)),
        dma((3, 4 * SUMS)),
    ]
    return pl.pallas_call(
        functools.partial(layer_kernel, sizes),
        out_shape=jax.ShapeDtypeStruct(tokens.shape, BF16),
        in_specs=[pl.BlockSpec(memory_space=pltpu.HBM)] * len(shaped),
        out_specs=pl.BlockSpec(memory_space=pl.ANY),
        scratch_shapes=scratch,
        compiler_params=pltpu.CompilerParams(
            collective_id=0, has_side_effects=True, vmem_limit_bytes=67_043_328
        ),
    )(*shaped)


def fits(mesh, args):
    tokens, val_weight, out_weight = args[0], args[2], args[6]
    up_gate_weight, down_weight = args[9], args[12]
    if (mesh.shape["grp"], mesh.shape["fs"], mesh.shape["tp"]) != (2, 4, 4):
        return False
    rows = tokens.shape[0] // 32
    local_ch, local_ff = val_weight.shape[1] // 4, up_gate_weight.shape[1] // 4
    local_model = tokens.shape[1] // 4
    return (
        rows % 16 == 0
        and local_model % (32 * UP_CUTS) == 0
        and local_ff % 128 == 0
        and 4 * rows % LEN == 0
        and local_ch % LANES == 0
        and local_ff % (2 * LANES) == 0
        and local_model % (SUMS * LANES) == 0
        and args[4].shape[0] <= 32
        and args[11].shape[1] <= 8
    )


def solution(mesh):
    specs = (
        P(("grp", "fs", "tp"), None),
        P(),
        P("fs", "tp"),
        P("fs", "tp"),
        P(),
        P(),
        P("tp", "fs"),
        P(),
        P(),
        P("fs", "tp"),
        P("fs", "tp"),
        P(),
        P("tp", "fs"),
        P(),
    )

    def whole(*args):
        body = run_kernel if fits(mesh, args) else plain
        step = jax.shard_map(
            body,
            mesh=mesh,
            in_specs=specs,
            out_specs=P(("grp", "fs", "tp"), None),
            check_vma=False,
        )
        return step(*args)

    return whole
```
